512 devices in a mesh: ep: 32 (over z, core), tp: 16 (over y, x).
Axes of the slice: x: 4, y: 4, z: 16, core: 2. Of those that a mesh axis runs over, the one named last changes fastest.
Arguments:
- tokens: bfloat16 [4096, 4096], P('ep', 'tp'), may hold values from -6 to 6
- out_grad: bfloat16 [4096, 4096], P('ep', 'tp'), may hold values from -1.5 to 1.5
- routes: int32 [4096, 2], P('ep'), may hold values from 0 to 31, all different within a row; in each aligned block of 128 rows (0 to 127, 128 to 255, ...) at most 10 rows name the same one
- route_weights: float32 [4096, 2], P('ep'), may hold values from 0.2 to 1.2
- gate_proj: bfloat16 [32, 1024, 4096], P('ep', 'tp'), may hold values from -0.09375 to 0.09375
- up_proj: bfloat16 [32, 1024, 4096], P('ep', 'tp'), may hold values from -0.09375 to 0.09375
- down_proj: bfloat16 [32, 1024, 4096], P('ep', 'tp'), may hold values from -0.1875 to 0.1875
- shared_hidden: bfloat16 [4096, 1024], P('ep'), may hold values from -6 to 6
Outputs:
- token_grad: bfloat16 [4096, 4096], P('ep', 'tp')
- weight_grad: float32 [4096, 2], P('ep')
- gate_grad: bfloat16 [32, 1024, 4096], P('ep', 'tp')
- up_grad: bfloat16 [32, 1024, 4096], P('ep', 'tp')
- down_grad: bfloat16 [32, 1024, 4096], P('ep', 'tp')
- shared_grad: float32 [1024, 4096], P('ep', 'tp')
The draws below stay inside these ranges and needn't reach their ends.
Inputs may be any that keep to these rules, and one draw needn't show every extreme that they name: Within each block of 128 consecutive tokens, no expert is named by more than 10 routes, and in some blocks one expert is named by exactly 10. The 2 experts of one token differ.
All inputs are finite; a program needn't handle non-finite values.
Results may differ from the reference program's by a relative error of at most 0.0065.
Values may be sent and summed in bfloat16 or wider, within the bound.
A program may use at most 64 MiB of HBM per device.

```python
import math
import jax
import jax.numpy as jnp
import numpy as np
from jax import lax

D = 4096
FE = 1024
FS = 1024
TOP = 2
TOK_DEV = 128
EXPERTS = 32
TOKENS = 4096
CAP = 10
N_EP = 32
N_TP = 16


def strengthened(array, key, source, target, parts, factor):
    owner, partner = [(jnp.arange(array.shape[position]) // (array.shape[position] // parts)).reshape([-1 if axis == position else 1 for axis in range(array.ndim)]) for position in (source, target)]
    chosen = jax.random.permutation(key, parts)[partner]
    strong = (owner == chosen) | (owner == (partner + parts // 2) % parts)
    return jnp.where(strong, factor * array, array)


def steps_of(rng, extent, split, smallest, top_value):
    def one(axis_at, parts):
        steps = jax.random.uniform(jax.random.fold_in(jax.random.fold_in(rng, 6), axis_at), (parts,), jnp.float32, smallest / len(split), top_value / len(split))
        return jnp.repeat(jnp.exp(steps), extent[axis_at] // parts).reshape((-1,) + (1,) * (len(extent) - axis_at - 1))

    gain = one(*split[0])
    for cut in split[1:]:
        gain = gain * one(*cut)
    return gain


def shared_out(rng, own, number, rows, number_of, top, bound, slope):
    sequence = jax.random.permutation(rng, number_of)
    heavy_load, common = portions_of(number_of, rows * top, bound, slope, True), portions_of(number_of, rows * top, bound, slope, False)
    places = jnp.arange(number_of)

    def named(lengths, rotation):
        used = int((lengths > 0).sum())
        fixed = max(1, used // 4)
        moved = fixed + (places - fixed + rotation * (used - fixed)) % max(1, number_of - fixed)
        return jnp.zeros((number_of,), jnp.int32).at[sequence[jnp.where(places < fixed, places, moved)]].set(jnp.asarray(lengths, jnp.int32))

    lengths = jnp.where(number % 4 == 0, named(heavy_load, number // 4), named(common, number - number // 4 - 1))
    mixed = jax.random.permutation(jax.random.fold_in(own, 3), number_of)
    source_of, taker = mixed[0:number_of // 2 * 2:2], mixed[1:number_of // 2 * 2:2]
    room = jnp.minimum(lengths[source_of] - 1, bound - lengths[taker]) // 2
    room = jnp.where((source_of == sequence[0]) | (taker == sequence[0]) | (lengths[taker] == 0), 0, jnp.maximum(room, 0))
    moved = jax.random.randint(jax.random.fold_in(own, 4), (number_of // 2,), 0, 1 << 20) % (room + 1)
    lengths = lengths.at[source_of].add(-moved).at[taker].add(moved)
    members = jnp.searchsorted(jnp.cumsum(lengths), jnp.arange(rows * top), side="right").astype(jnp.int32)
    table = members.reshape(top, rows).T
    table = table[jax.random.permutation(jax.random.fold_in(own, 1), rows)]
    rotation = jax.random.randint(jax.random.fold_in(own, 2), (rows, 1), 0, top)
    return jnp.take_along_axis(table, (jnp.arange(top)[None, :] + rotation) % top, axis=1)


def portions_of(amount, total, bound, slope, full):
    loads = [(1 << 20) // math.isqrt(grade ** slope) + 1 for grade in range(1, amount + 1)]
    largest = bound if full else min(bound, max(-(-total // amount), total * loads[0] // sum(loads)))
    least = 1 if total - largest >= amount - 1 else 0
    holding, spare = [largest] + [least] * (amount - 1), total - largest - least * (amount - 1)
    while spare > 0:
        free = [i for i in range(1, amount) if holding[i] < largest] or [i for i in range(1, amount) if holding[i] < bound]
        mass, remaining = sum([loads[i] for i in free]), spare
        for i in free:
            addition = min(bound - holding[i], max(1, remaining * loads[i] // mass), spare)
            holding[i] = holding[i] + addition
            spare = spare - addition
    return np.array(holding)


def bell_draw(rng, extent, spread, bound, split=(), held_as=jnp.bfloat16):
    level = steps_of(rng, extent, split, -0.22, 0.18) if split else 1.0
    array = jax.random.normal(rng, extent, jnp.float32) * spread * level
    return jnp.minimum(jnp.maximum(array, -bound), bound).astype(held_as)


def gaussian_with(key, extent, scale, most, cuts, heavy, kind=jnp.bfloat16):
    result = scale * jax.random.normal(key, extent, jnp.float32)
    if cuts:
        result = result * steps_of(key, extent, cuts, -0.22, 0.18)
    return jnp.clip(strengthened(result, jax.random.fold_in(key, 3), *heavy), -most, most).astype(kind)


def setup_inputs(seed: int = 0) -> dict:
    streams_of = jax.random.split(jax.random.key(seed), 9)
    tokens = bell_draw(streams_of[0], (TOKENS, D), 1.0, 6.0, ((0, 32), (1, 16)))
    out_grad = bell_draw(streams_of[1], (TOKENS, D), 0.25, 1.5, ((0, 32), (1, 16)))
    routes_keys = jax.random.split(jax.random.fold_in(streams_of[2], 1), TOKENS // TOK_DEV)
    routes_turns = jax.random.permutation(jax.random.fold_in(streams_of[2], 3), TOKENS // TOK_DEV)
    routes = jax.vmap(lambda own, number: shared_out(jax.random.fold_in(streams_of[2], 2), own, number, TOK_DEV, EXPERTS, TOP, CAP, 2))(routes_keys, routes_turns).reshape((TOKENS, TOP))
    route_weights = jnp.clip(0.2 + 1 * jax.random.uniform(streams_of[3], (TOKENS, TOP), jnp.float32) ** steps_of(streams_of[3], (TOKENS, TOP), ((0, 32),), -0.2, 0.2), 0.2, 1.2)
    gate_proj = bell_draw(streams_of[4], (EXPERTS, FE, D), D ** -0.5, 0.09375, ((0, 32), (1, 16)))
    up_proj = bell_draw(streams_of[5], (EXPERTS, FE, D), D ** -0.5, 0.09375, ((0, 32), (1, 16)))
    down_proj = bell_draw(streams_of[6], (EXPERTS, FE, D), FE ** -0.5, 0.1875, ((0, 32), (1, 16)))
    shared_hidden = gaussian_with(streams_of[7], (TOKENS, FS), 1.0, 6.0, ((0, 32),), (0, 1, 32, 2.75))
    return {"tokens": tokens, "out_grad": out_grad, "routes": routes, "route_weights": route_weights, "gate_proj": gate_proj, "up_proj": up_proj, "down_proj": down_proj, "shared_hidden": shared_hidden}


def reference(tokens, out_grad, routes, route_weights, gate_proj, up_proj, down_proj, shared_hidden):
    block_routes = TOK_DEV * TOP
    expert_rows = N_EP * CAP
    flat_routes = routes.reshape(N_EP, block_routes)
    expert_ids = jnp.arange(EXPERTS, dtype=jnp.int32)
    onehot = (flat_routes[:, :, None] == expert_ids[None, None, :]).astype(jnp.int32)
    slot_rank = jnp.sum((jnp.cumsum(onehot, axis=1) - 1) * onehot, axis=2)
    block_ids = jnp.arange(N_EP, dtype=jnp.int32)[:, None]
    slot_index = (flat_routes * expert_rows + block_ids * CAP + slot_rank).reshape(-1).astype(jnp.int32)
    route_ids = jnp.arange(TOKENS * TOP, dtype=jnp.int32)
    route_of_slot = jnp.full((EXPERTS * expert_rows,), -1, jnp.int32).at[slot_index].set(route_ids)
    filled = route_of_slot >= 0
    safe_route = jnp.maximum(route_of_slot, 0).astype(jnp.int32)
    token_of_slot = (safe_route // TOP).astype(jnp.int32)
    weight_b = lax.optimization_barrier(route_weights.reshape(-1).astype(jnp.bfloat16)).astype(jnp.float32)
    slot_weight = jnp.where(filled, weight_b[safe_route], jnp.zeros((), jnp.float32))
    zero_value = jnp.zeros((), jnp.bfloat16)
    slot_tokens = jnp.where(filled[:, None], tokens[token_of_slot], zero_value).reshape(EXPERTS, expert_rows, D)
    slot_grads = jnp.where(filled[:, None], out_grad[token_of_slot], zero_value).reshape(EXPERTS, expert_rows, D)
    slot_scale = slot_weight.reshape(EXPERTS, expert_rows)
    block_width = FE // N_TP
    contract_features = (((1,), (1,)), ((), ()))
    contract_rows = (((0,), (0,)), ((), ()))

    def one_expert(operands):
        rows_in, grads_in, scale, gate_matrix, up_matrix, down_matrix = operands
        pre_gate = lax.dot_general(rows_in, gate_matrix, contract_features, preferred_element_type=jnp.float32)
        pre_up = lax.dot_general(rows_in, up_matrix, contract_features, preferred_element_type=jnp.float32)
        squash = jax.nn.sigmoid(pre_gate)
        activated = pre_gate * squash
        hidden = lax.optimization_barrier((activated * pre_up).astype(jnp.bfloat16))
        back_grad = lax.dot_general(grads_in, down_matrix, contract_features,
                                    preferred_element_type=jnp.float32)
        products = jnp.sum(hidden.astype(jnp.float32) * back_grad, axis=1)
        hidden_grad = scale[:, None] * back_grad
        scaled_hidden = (scale[:, None] * hidden.astype(jnp.float32)).astype(jnp.bfloat16)
        gate_delta = (hidden_grad * pre_up * squash * (1.0 + pre_gate * (1.0 - squash))).astype(jnp.bfloat16)
        up_delta = (hidden_grad * activated).astype(jnp.bfloat16)
        gate_part = lax.dot_general(gate_delta, rows_in, contract_rows,
                                    preferred_element_type=jnp.float32).astype(jnp.bfloat16)
        up_part = lax.dot_general(up_delta, rows_in, contract_rows,
                                  preferred_element_type=jnp.float32).astype(jnp.bfloat16)
        down_part = lax.dot_general(scaled_hidden, grads_in, contract_rows,
                                    preferred_element_type=jnp.float32).astype(jnp.bfloat16)
        gate_blocks = gate_delta.astype(jnp.float32).reshape(-1, N_TP, block_width)
        up_blocks = up_delta.astype(jnp.float32).reshape(-1, N_TP, block_width)
        gate_weights = gate_matrix.astype(jnp.float32).reshape(N_TP, block_width, D)
        up_weights = up_matrix.astype(jnp.float32).reshape(N_TP, block_width, D)
        block_part = jnp.einsum('rtf,tfd->trd', gate_blocks, gate_weights) + jnp.einsum('rtf,tfd->trd', up_blocks, up_weights)
        block_part = lax.optimization_barrier(block_part.astype(jnp.bfloat16)).astype(jnp.float32)
        return jnp.sum(block_part, axis=0), products, gate_part, up_part, down_part

    route_rows, products, gate_grad, up_grad, down_grad = lax.map(
        one_expert, (slot_tokens, slot_grads, slot_scale, gate_proj, up_proj, down_proj))
    route_rows = route_rows.reshape(EXPERTS * expert_rows, D)
    products = products.reshape(-1)
    token_grad = jnp.sum(route_rows[slot_index].reshape(TOKENS, TOP, D), axis=1).astype(jnp.bfloat16)
    weight_grad = products[slot_index].reshape(TOKENS, TOP)
    shared_grad = lax.dot_general(shared_hidden, out_grad, (((0,), (0,)), ((), ())),
                                  preferred_element_type=jnp.float32)
    return token_grad, weight_grad, gate_grad, up_grad, down_grad, shared_grad
```

```python
import functools

import jax
import jax.numpy as jnp
from jax import lax
from jax.experimental import pallas as pl
from jax.experimental.pallas import tpu as pltpu
from jax.sharding import PartitionSpec as P

MESH = pl.DeviceIdType.MESH
BF = jnp.bfloat16
F32 = jnp.float32
SIDE = 4
HIGH = lax.Precision.HIGHEST


def dot(a, b, da, db, precision=None):
    return lax.dot_general(
        a, b, (((da,), (db,)), ((), ())), preferred_element_type=F32, precision=precision
    )


def iota(shape, dim):
    return lax.broadcasted_iota(jnp.int32, shape, dim)


def kernel(
    zs, cap,
    tok, og, routes, routes_t, rw, rw_t, gate, up, down, sh,
    tg_o, wg_o, gg_o, ug_o, dg_o, sg_o,
    wgu, wdn, sb, xa, dl, hd, dlt, hdt, pr, r1, f1, s0, s1, r2, f2, rt, rh, pb, pz, ph, cm,
    sp, sc, shb, shs,
    w_sem, z_send, z_recv, ag_send, ag_recv, rs_send, rs_recv, rz_send, rz_recv,
    pb_send, pb_recv, pz_send, pz_recv, sc_send, sc_recv, sh_send, sh_recv,
):
    ep, tp = lax.axis_index("ep"), lax.axis_index("tp")
    z, c = ep // 2, lax.rem(ep, 2)
    yx = (tp // SIDE, lax.rem(tp, SIDE))
    n_tp = SIDE * SIDE
    slots = 2 * zs
    rows = slots * cap
    half = rows // 2
    pairs = cap // 2
    quarter = zs // 4
    fe = gate.shape[0]
    n_tok = tok.shape[0]

    def ring(d):
        return lax.rem(z + d + zs, zs)

    def ep_of(d, cd):
        return ring(d) * 2 + lax.rem(c + cd, 2)

    def tp_of(h, dp, ds):
        dy, dx = (ds, dp) if h == 0 else (dp, ds)
        return lax.rem(yx[0] + dy + SIDE, SIDE) * SIDE + lax.rem(yx[1] + dx + SIDE, SIDE)

    def remote(src, dst, ssem, rsem, dev):
        return pltpu.make_async_remote_copy(
            src_ref=src, dst_ref=dst, send_sem=ssem, recv_sem=rsem,
            device_id=dev, device_id_type=MESH,
        )

    def arrived(ref, sem):
        remote(ref, ref, sem, sem, (ep, tp)).wait_recv()

    def left(ref, sem):
        remote(ref, ref, sem, sem, (ep, tp)).wait_send()

    loads = [
        pltpu.make_async_copy(gate, wgu.at[pl.ds(0, fe)], w_sem.at[0]),
        pltpu.make_async_copy(up, wgu.at[pl.ds(fe, fe)], w_sem.at[1]),
        pltpu.make_async_copy(down, wdn, w_sem.at[2]),
    ]
    for load in loads:
        load.start()

    barrier = pltpu.get_barrier_semaphore()
    for d in range(zs):
        for cd in range(2):
            if d or cd:
                pl.semaphore_signal(barrier, inc=1, device_id=(ep_of(d, cd), tp), device_id_type=MESH)
    for dy in range(SIDE):
        for dx in range(SIDE):
            if dy or dx:
                pl.semaphore_signal(barrier, inc=1, device_id=(ep, tp_of(0, dx, dy)), device_id_type=MESH)

    def tables(shape, dim):
        r = iota(shape, dim)
        j = lax.shift_right_logical(r * (65536 // cap + 1), 16)
        e = lax.bitwise_and(z + lax.shift_right_logical(j, 1), zs - 1) * 2 + lax.bitwise_and(c + j, 1)
        return e, (r - cap * j).astype(F32)

    def flag(m):
        return jnp.where(m, 1.0, 0.0).astype(BF)

    def weight(x):
        return x.astype(BF).astype(F32)

    before = flag(iota((n_tok, n_tok), 0) < iota((n_tok, n_tok), 1))
    after = flag(iota((n_tok, n_tok), 0) > iota((n_tok, n_tok), 1))
    e, s = tables((rows, n_tok), 0)
    first = routes_t[0:1, :] == e
    hit = first | (routes_t[1:2, :] == e)
    chosen = hit & (dot(flag(hit), before, 1, 0) == s)
    wt = weight(rw_t[...])
    slot_w = jnp.sum(jnp.where(chosen, jnp.where(first, wt[0:1, :], wt[1:2, :]), 0.0), axis=1, keepdims=True)
    pick = flag(chosen)
    sbv = sb.reshape(4, rows, 128)
    for g in range(2):
        sbv[g] = dot(pick, tok[:, g * 128 : (g + 1) * 128], 1, 0).astype(BF)
        sbv[2 + g] = (slot_w * dot(pick, og[:, g * 128 : (g + 1) * 128], 1, 0)).astype(BF)

    pl.semaphore_wait(barrier, slots - 1 + n_tp - 1)

    def order(chunk):
        ds = [quarter - q for q in range(zs // 2)] if chunk == 0 else [quarter - q for q in range(zs // 2, zs)]
        ds = [(d + zs // 2 - 1) % zs - (zs // 2 - 1) for d in ds]
        return sorted(ds, key=abs)

    def slot_in(d, cd):
        return ((quarter - d) % zs) * 2 + cd - (0 if (quarter - d) % zs < zs // 2 else slots // 2)

    def exchange(chunk):
        for d in order(chunk):
            for cd in (1, 0):
                if d or cd:
                    j = (d % zs) * 2 + cd
                    remote(
                        sb.at[:, pl.ds(j * pairs, pairs)],
                        xa.at[chunk, tp, :, pl.ds(slot_in(d, cd) * pairs, pairs)],
                        z_send, z_recv.at[chunk], (ep_of(d, cd), tp),
                    ).start()

    exchange(0)
    exchange(1)
    xa[0, tp, :, pl.ds(slot_in(0, 0) * pairs, pairs)] = sb[:, pl.ds(0, pairs)]

    share = sg_o.shape[0]
    for b in range(sp.shape[0]):
        for cc in range(2):
            lo = (b * 2 + cc) * share
            if lo % 128 == 0:
                wide = dot(sh[:, lo : lo + 128], og[...], 0, 0)
            sp[b, cc] = wide[lo % 128 : lo % 128 + share]
    remote(sp.at[:, 1 - c], sc, sc_send, sc_recv, (ep_of(0, 1), tp)).start()

    def term(d):
        zz = ring(d)
        return sp[zz, c] + sc[zz]

    far = zs // 2

    def shared(step):
        if step == 0:
            arrived(sc, sc_recv)
        for way, hops in ((0, far), (1, far - 1)):
            sign = 1 if way == 0 else -1
            if step > hops:
                continue
            total = term(sign * (hops - step))
            if step:
                arrived(shb.at[way, step - 1], sh_recv.at[way, step - 1])
                total = total + shb[way, step - 1]
            if step < hops:
                shs[way, step] = total
                remote(
                    shs.at[way, step], shb.at[way, step], sh_send.at[way, step], sh_recv.at[way, step],
                    (ep_of(sign, 0), tp),
                ).start()
            elif way == 1:
                sg_o[...] = total
            else:
                sg_o[...] = sg_o[...] + total - term(0)

    back = (0, -1, 1, 2)

    def gather_send(ch, h, k, kind, t, g0, gn, dev_t):
        ref = xa.at[ch, t, pl.ds(2 * h + g0, gn)]
        remote(ref, ref, ag_send, ag_recv.at[ch, h, k, kind], (ep, dev_t)).start()

    def gather_wait(ch, h, k, kind, g0, gn):
        arrived(xa.at[ch, 0, pl.ds(2 * h + g0, gn)], ag_recv.at[ch, h, k, kind])

    def spread(ch, h, k):
        t = tp_of(h, back[k], 0)
        gather_send(ch, h, k, 0, t, 0, 2, tp_of(h, 0, 1))
        gather_send(ch, h, k, 1, t, 0, 2, tp_of(h, 0, -1))

    def relay(ch, h, k):
        gather_wait(ch, h, k, 0, 0, 2)
        gather_send(ch, h, k, 2, tp_of(h, back[k], -1), 0, 1, tp_of(h, 0, 1))
        gather_wait(ch, h, k, 1, 0, 2)
        gather_send(ch, h, k, 3, tp_of(h, back[k], 1), 1, 1, tp_of(h, 0, -1))

    def g_0(ch):
        arrived(xa.at[ch, 0, :, pl.ds(0, (slots // 2 - (1 if ch == 0 else 0)) * pairs)], z_recv.at[ch])
        for h in range(2):
            gather_send(ch, h, 4, 0, tp, 0, 2, tp_of(h, 1, 0))
            gather_send(ch, h, 4, 1, tp, 0, 2, tp_of(h, -1, 0))
        for h in range(2):
            spread(ch, h, 0)

    def g_1(ch):
        for h in range(2):
            gather_wait(ch, h, 4, 0, 0, 2)
            gather_send(ch, h, 4, 2, tp_of(h, -1, 0), 0, 1, tp_of(h, 1, 0))
            gather_wait(ch, h, 4, 1, 0, 2)
            gather_send(ch, h, 4, 3, tp_of(h, 1, 0), 1, 1, tp_of(h, -1, 0))
        for h in range(2):
            spread(ch, h, 1)
            spread(ch, h, 2)

    def g_2(ch):
        for h in range(2):
            relay(ch, h, 0)
        for h in range(2):
            gather_wait(ch, h, 4, 2, 0, 1)
            gather_wait(ch, h, 4, 3, 1, 1)
            spread(ch, h, 3)

    def g_3(ch):
        for h in range(2):
            relay(ch, h, 1)
            relay(ch, h, 2)

    def g_4(ch):
        for h in range(2):
            relay(ch, h, 3)

    def g_5(ch):
        for h in range(2):
            for k in range(4):
                gather_wait(ch, h, k, 2, 0, 1)
                gather_wait(ch, h, k, 3, 1, 1)

    xav = xa.reshape(2, n_tp, 4, half, 128)
    width = 256

    def expert(ch):
        def sums(i, total):
            a, b = total
            for u in range(4):
                t = i * 4 + u
                cols = pl.ds(pl.multiple_of(t * width, width), width)
                x = jnp.concatenate([xav[ch, t, 0], xav[ch, t, 1]], axis=1)
                y = jnp.concatenate([xav[ch, t, 2], xav[ch, t, 3]], axis=1)
                a = a + dot(x, wgu[:, cols], 1, 1)
                b = b + dot(y, wdn[:, cols], 1, 1)
            return a, b

        start = (jnp.zeros((half, 2 * fe), F32), jnp.zeros((half, fe), F32))
        gu, back_grad = lax.fori_loop(0, n_tp // 4, sums, start)
        pre_gate, pre_up = gu[:, :fe], gu[:, fe:]
        squash = 1.0 / (1.0 + jnp.exp(-pre_gate))
        activated = pre_gate * squash
        hidden = (activated * pre_up).astype(BF)
        gate_delta = back_grad * pre_up * squash * (1.0 + pre_gate * (1.0 - squash))
        at = pl.ds(ch * half, half)
        deltas = jnp.concatenate([gate_delta, back_grad * activated], axis=1)
        dl[at, :] = deltas.astype(BF)
        hd[at, :] = hidden
        product = hidden.astype(F32) * back_grad
        line = dot(jnp.ones((8, fe), F32), product, 1, 1, HIGH)
        pb[tp, pl.ds(ch, 1), pl.ds(0, half)] = line[0:1]

    def parts(ch):
        at = pl.ds(ch * half, half)
        for dy in range(SIDE):
            for dx in range(SIDE):
                t = tp_of(0, dx, dy)
                cols = pl.ds(pl.multiple_of(t * width, width), width)
                out = dot(dl[at, :], wgu[:, cols], 1, 0).astype(BF)
                pr[ch, 0, dx, dy] = out[:, :128]
                pr[ch, 1, dy, dx] = out[:, 128:]

    def add(*xs):
        total = xs[0].astype(F32)
        for x in xs[1:]:
            total = total + x.astype(F32)
        return total

    def sum_send(ch, h, src, buf, i, base, dev_t):
        remote(src, buf.at[ch, h, i], rs_send.at[base // 6], rs_recv.at[ch, h, base + i], (ep, dev_t)).start()

    def sum_wait(ch, h, buf, i, base):
        arrived(buf.at[ch, h, i], rs_recv.at[ch, h, base + i])

    lo, hi = pl.ds(0, 2), pl.ds(2, 2)
    top, low = pl.ds(0, half // 2), pl.ds(half // 2, half // 2)

    def q_0(ch):
        for h in range(2):
            sum_send(ch, h, pr.at[ch, h, 2, lo], r1, 0, 0, tp_of(h, 1, 0))
            sum_send(ch, h, pr.at[ch, h, 2, hi], r1, 1, 0, tp_of(h, -1, 0))
        for h in range(2):
            sum_send(ch, h, pr.at[ch, h, 1, hi], r1, 2, 0, tp_of(h, 1, 0))
            sum_send(ch, h, pr.at[ch, h, 3, lo], r1, 3, 0, tp_of(h, -1, 0))

    def q_1(ch):
        for h in range(2):
            sum_wait(ch, h, r1, 0, 0)
            f1[ch, h, 0] = add(pr[ch, h, 1, lo], r1[ch, h, 0]).astype(BF)
            sum_send(ch, h, f1.at[ch, h, 0], r1, 4, 0, tp_of(h, 1, 0))
            sum_wait(ch, h, r1, 1, 0)
            f1[ch, h, 1] = add(pr[ch, h, 3, hi], r1[ch, h, 1]).astype(BF)
            sum_send(ch, h, f1.at[ch, h, 1], r1, 5, 0, tp_of(h, -1, 0))

    def q_2(ch):
        for h in range(2):
            for i in (3, 2, 4, 5):
                sum_wait(ch, h, r1, i, 0)
            for ds in (2, 1, 3, 0):
                pair = (4, 3) if ds < 2 else (2, 5)
                total = add(pr[ch, h, 0, ds], r1[ch, h, pair[0], ds % 2], r1[ch, h, pair[1], ds % 2])
                if ds:
                    s1[ch, h, ds - 1] = total.astype(BF)
                else:
                    s0[ch, h] = total
            sum_send(ch, h, s1.at[ch, h, 1, top], r2, 0, 6, tp_of(h, 0, 1))
            sum_send(ch, h, s1.at[ch, h, 1, low], r2, 1, 6, tp_of(h, 0, -1))
            sum_send(ch, h, s1.at[ch, h, 0, low], r2, 2, 6, tp_of(h, 0, 1))
            sum_send(ch, h, s1.at[ch, h, 2, top], r2, 3, 6, tp_of(h, 0, -1))

    def q_3(ch):
        for h in range(2):
            sum_wait(ch, h, r2, 0, 6)
            f2[ch, h, 0] = add(s1[ch, h, 0, top], r2[ch, h, 0]).astype(BF)
            sum_send(ch, h, f2.at[ch, h, 0], r2, 4, 6, tp_of(h, 0, 1))
            sum_wait(ch, h, r2, 1, 6)
            f2[ch, h, 1] = add(s1[ch, h, 2, low], r2[ch, h, 1]).astype(BF)
            sum_send(ch, h, f2.at[ch, h, 1], r2, 5, 6, tp_of(h, 0, -1))

    rtv = rt.reshape(2, 2, half, 128)

    def q_4(ch):
        for h in range(2):
            for i in (3, 2, 4, 5):
                sum_wait(ch, h, r2, i, 6)
            rtv[ch, h, top] = add(s0[ch, h, top], r2[ch, h, 4], r2[ch, h, 3]).astype(BF)
            rtv[ch, h, low] = add(s0[ch, h, low], r2[ch, h, 2], r2[ch, h, 5]).astype(BF)
        for d in order(ch)[::-1]:
            for cd in (1, 0):
                here = pl.ds(slot_in(d, cd) * pairs, pairs)
                there = pl.ds(((d % zs) * 2 + cd) * pairs, pairs)
                if d or cd:
                    remote(
                        rt.at[ch, :, here], rh.at[:, there], rz_send, rz_recv, (ep_of(-d, cd), tp)
                    ).start()
                else:
                    rh[:, there] = rt[ch, :, here]

    def product_send():
        for dy in range(SIDE):
            for dx in range(SIDE):
                if dy or dx:
                    remote(pb.at[tp], pb.at[tp], pb_send, pb_recv, (ep, tp_of(0, dx, dy))).start()

    def product_return():
        arrived(pb.at[pl.ds(0, n_tp - 1)], pb_recv)
        for ch in range(2):
            total = pb[0, pl.ds(ch, 1), pl.ds(0, half)]
            for t in range(1, n_tp):
                total = total + pb[t, pl.ds(ch, 1), pl.ds(0, half)]
            r = iota((slots // 2, half), 1)
            j = lax.shift_right_logical(r * (65536 // cap + 1), 16)
            own = jnp.where(j == iota((slots // 2, half), 0), total, 0.0)
            r = iota((half, 128), 0)
            j = lax.shift_right_logical(r * (65536 // cap + 1), 16)
            lane = jnp.where(r - cap * j == iota((half, 128), 1), 1.0, 0.0)
            table = dot(own, lane, 1, 0, HIGH)
            for i in range(slots // 2):
                pz[ch * (slots // 2) + i] = table[i : i + 1]
        for ch in range(2):
            for d in order(ch)[::-1]:
                for cd in (1, 0):
                    i, j = ch * (slots // 2) + slot_in(d, cd), (d % zs) * 2 + cd
                    if d or cd:
                        remote(pz.at[i], ph.at[j], pz_send, pz_recv, (ep_of(-d, cd), tp)).start()
                    else:
                        ph[j] = pz[i]

    def weight_grads(t0, t1):
        def one(t, carry):
            cols = pl.ds(pl.multiple_of(t * width, width), width)
            both = jnp.zeros((2 * fe, width), F32)
            last = jnp.zeros((fe, width), F32)
            for ch in range(2):
                x = jnp.concatenate([xav[ch, t, 0], xav[ch, t, 1]], axis=1)
                y = jnp.concatenate([xav[ch, t, 2], xav[ch, t, 3]], axis=1)
                both = both + dot(dlt[ch], x, 1, 0)
                last = last + dot(hdt[ch], y, 1, 0)
            gg_o[:, cols] = both[:fe].astype(BF)
            ug_o[:, cols] = both[fe:].astype(BF)
            dg_o[:, cols] = last.astype(BF)
            return carry

        lax.fori_loop(t0, t1, one, 0)

    def turned(ch):
        at = pl.ds(ch * half, half)
        dlt[ch] = dl[at, :].astype(F32).T.astype(BF)
        hdt[ch] = hd[at, :].astype(F32).T.astype(BF)

    g_0(0)
    shared(0)
    g_1(0)
    shared(1)
    g_2(0)
    shared(2)
    g_0(1)
    shared(3)
    g_3(0)
    g_1(1)
    shared(4)
    g_4(0)
    g_5(0)
    for load in loads:
        load.wait()
    expert(0)
    shared(5)
    g_2(1)
    parts(0)
    g_3(1)
    shared(6)
    turned(0)
    g_4(1)
    q_0(0)
    shared(7)
    g_5(1)
    expert(1)
    product_send()
    q_1(0)
    parts(1)
    q_0(1)
    shared(8)
    turned(1)
    q_2(0)
    weight_grads(0, 4)
    q_1(1)
    q_3(0)
    weight_grads(4, 7)
    q_4(0)
    q_2(1)
    product_return()
    weight_grads(7, 11)
    q_3(1)
    weight_grads(11, 13)
    q_4(1)
    weight_grads(13, 16)

    e, s = tables((n_tok, rows), 1)
    r0, r1c = routes[:, 0:1], routes[:, 1:2]
    hit = (r0 == e) | (r1c == e)
    cm[...] = flag(hit & (dot(after, flag(hit), 1, 0) == s))
    j = iota((n_tok, slots), 1)
    ej = lax.bitwise_and(z + lax.shift_right_logical(j, 1), zs - 1) * 2 + lax.bitwise_and(c + j, 1)
    seen = dot(after, flag((r0 == ej) | (r1c == ej)), 1, 0)
    wc = weight(rw[...])
    arrived(ph.at[pl.ds(0, slots - 1)], pz_recv)
    table = jnp.concatenate([ph[i] for i in range(slots)], axis=0)
    for k in range(2):
        mine = routes[:, k : k + 1] == ej
        rank = jnp.sum(jnp.where(mine, seen, 0.0), axis=1, keepdims=True)
        found = dot(jnp.where(mine, 1.0, 0.0), table, 1, 0, HIGH)
        lane = iota((n_tok, 128), 1).astype(F32)
        value = jnp.sum(jnp.where(lane == rank, found, 0.0), axis=1, keepdims=True)
        wg_o[:, k : k + 1] = value / wc[:, k : k + 1]
    arrived(rh.at[:, pl.ds(0, (slots - 1) * pairs)], rz_recv)
    rhv = rh.reshape(2, rows, 128)
    for h in range(2):
        tg_o[:, h * 128 : (h + 1) * 128] = dot(cm[...], rhv[h], 1, 0).astype(BF)

    left(sb.at[:, pl.ds(0, (slots - 1) * pairs)], z_send)
    left(xa.at[:, pl.ds(0, n_tp - 1)], ag_send)
    left(r1, rs_send.at[0])
    left(r2, rs_send.at[1])
    left(rh.at[:, pl.ds(0, (slots - 1) * pairs)], rz_send)
    left(pb.at[pl.ds(0, n_tp - 1)], pb_send)
    left(ph.at[pl.ds(0, slots - 1)], pz_send)
    left(sc, sc_send)
    for way, hops in ((0, far), (1, far - 1)):
        for step in range(hops):
            left(shs.at[way, step], sh_send.at[way, step])


def local(zs, tokens, out_grad, routes, route_weights, gate_proj, up_proj, down_proj, shared_hidden):
    n_tok, feat = tokens.shape
    _, fe, width = gate_proj.shape
    slots = 2 * zs
    cap = max(2, 5 * n_tok * routes.shape[1] // (4 * slots))
    rows = slots * cap
    half = rows // 2
    n_tp = SIDE * SIDE
    share = shared_hidden.shape[1] // slots
    far = zs // 2
    vmem = pl.BlockSpec(memory_space=pltpu.VMEM)
    hbm = pl.BlockSpec(memory_space=pl.ANY)
    dma = pltpu.SemaphoreType.DMA
    V = pltpu.VMEM
    out = pl.pallas_call(
        functools.partial(kernel, zs, cap),
        out_shape=(
            jax.ShapeDtypeStruct((n_tok, feat), BF),
            jax.ShapeDtypeStruct((n_tok, 2), F32),
            jax.ShapeDtypeStruct((fe, width), BF),
            jax.ShapeDtypeStruct((fe, width), BF),
            jax.ShapeDtypeStruct((fe, width), BF),
            jax.ShapeDtypeStruct((share, feat), F32),
        ),
        in_specs=[vmem] * 6 + [hbm] * 3 + [vmem],
        out_specs=(vmem,) * 6,
        scratch_shapes=[
            V((2 * fe, width), BF),
            V((fe, width), BF),
            V((4, rows // 2, 2, 128), BF),
            V((2, n_tp, 4, half // 2, 2, 128), BF),
            V((rows, 2 * fe), BF),
            V((rows, fe), BF),
            V((2, 2 * fe, half), BF),
            V((2, fe, half), BF),
            V((2, 2, SIDE, SIDE, half, 128), BF),
            V((2, 2, 6, 2, half, 128), BF),
            V((2, 2, 2, 2, half, 128), BF),
            V((2, 2, half, 128), F32),
            V((2, 2, 3, half, 128), BF),
            V((2, 2, 6, half // 2, 128), BF),
            V((2, 2, 2, half // 2, 128), BF),
            V((2, 2, half // 2, 2, 128), BF),
            V((2, rows // 2, 2, 128), BF),
            V((n_tp, 2, 256), F32),
            V((slots, 1, 128), F32),
            V((slots, 1, 128), F32),
            V((n_tok, rows), BF),
            V((zs, 2, share, feat), F32),
            V((zs, share, feat), F32),
            V((2, far, share, feat), F32),
            V((2, far, share, feat), F32),
            dma((3,)),
            dma, dma((2,)),
            dma, dma((2, 2, 5, 4)),
            dma((2,)), dma((2, 2, 12)),
            dma, dma,
            dma, dma,
            dma, dma,
            dma, dma,
            dma((2, far)), dma((2, far)),
        ],
        compiler_params=pltpu.CompilerParams(collective_id=0, has_side_effects=True),
    )(
        tokens, out_grad, routes, routes.T, route_weights, route_weights.T,
        gate_proj[0], up_proj[0], down_proj[0], shared_hidden,
    )
    tg, wg, gg, ug, dg, sg = out
    return tg, wg, gg[None], ug[None], dg[None], sg


def solution(mesh):
    zs = mesh.shape["ep"] // 2
    features, whole, weights = P("ep", "tp"), P("ep", None), P("ep", "tp", None)
    return jax.shard_map(
        functools.partial(local, zs),
        mesh=mesh,
        in_specs=(features, features, whole, whole, weights, weights, weights, whole),
        out_specs=(features, whole, weights, weights, weights, features),
        check_vma=False,
    )
```

```python
import functools

import jax
import jax.numpy as jnp
from jax import lax
from jax.experimental import pallas as pl
from jax.experimental.pallas import tpu as pltpu
from jax.sharding import PartitionSpec as P

MESH = pl.DeviceIdType.MESH
BF = jnp.bfloat16
F32 = jnp.float32
SIDE = 4
ORDER = (0, 1, 2, 3)
HIGH = lax.Precision.HIGHEST


def chunks_of(zs):
    near = sorted(range(1 - zs // 2, zs // 2 + 1), key=lambda d: (abs(d), -d))
    size = zs // len(ORDER)
    parts = [near[k * size : (k + 1) * size] for k in range(len(ORDER))]
    return [parts[k] for k in ORDER]


def dot(a, b, da, db, precision=None):
    return lax.dot_general(
        a, b, (((da,), (db,)), ((), ())), preferred_element_type=F32, precision=precision
    )


def iota(shape, dim):
    return lax.broadcasted_iota(jnp.int32, shape, dim)


def kernel(
    zs, cap,
    tok_h, og_h, routes_h, rw_h, gate, up, down, sh_h,
    tg_o, wg_o, gg_o, ug_o, dg_o, sg_o,
    tok, og, routes_t, rw_t, sh, wgu, wdn, sb, xa, dl, hd, dlt, hdt, pr, r1, f1, s0, s1, r2t, r2l, f2t, f2l, rt, rh, pb, pz, ph, cm,
    sp, sc, shb, shs,
    w_sem, z_send, z_recv, ag_send, ag_recv, rs_send, rs_recv, rz_send, rz_recv,
    pb_send, pb_recv, pz_send, pz_recv, sc_send, sc_recv, sh_send, sh_recv,
):
    ep, tp = lax.axis_index("ep"), lax.axis_index("tp")
    z, c = ep // 2, lax.rem(ep, 2)
    yx = (tp // SIDE, lax.rem(tp, SIDE))
    n_tp = SIDE * SIDE
    slots = 2 * zs
    rows = slots * cap
    groups = chunks_of(zs)
    nch = len(groups)
    ns = slots // nch
    half = rows // nch
    cut = (half // 2 + 15) // 16 * 16
    pairs = cap // 2
    fe = gate.shape[0]
    n_tok = tok.shape[0]

    def ring(d):
        return lax.rem(z + d + zs, zs)

    def ep_of(d, cd):
        return ring(d) * 2 + lax.rem(c + cd, 2)

    def tp_of(h, dp, ds):
        dy, dx = (ds, dp) if h == 0 else (dp, ds)
        return lax.rem(yx[0] + dy + SIDE, SIDE) * SIDE + lax.rem(yx[1] + dx + SIDE, SIDE)

    def remote(src, dst, ssem, rsem, dev):
        return pltpu.make_async_remote_copy(
            src_ref=src, dst_ref=dst, send_sem=ssem, recv_sem=rsem,
            device_id=dev, device_id_type=MESH,
        )

    def arrived(ref, sem):
        remote(ref, ref, sem, sem, (ep, tp)).wait_recv()

    def left(ref, sem):
        remote(ref, ref, sem, sem, (ep, tp)).wait_send()

    loads = [
        pltpu.make_async_copy(gate, wgu.at[pl.ds(0, fe)], w_sem.at[0]),
        pltpu.make_async_copy(up, wgu.at[pl.ds(fe, fe)], w_sem.at[1]),
        pltpu.make_async_copy(down, wdn, w_sem.at[2]),
    ]
    small = [
        pltpu.make_async_copy(src, dst, w_sem.at[3 + i])
        for i, (src, dst) in enumerate(
            ((routes_h, routes_t), (rw_h, rw_t), (tok_h, tok), (og_h, og), (sh_h, sh))
        )
    ]
    for load in small + loads:
        load.start()

    barrier = pltpu.get_barrier_semaphore()
    for d in range(zs):
        for cd in range(2):
            if d or cd:
                pl.semaphore_signal(barrier, inc=1, device_id=(ep_of(d, cd), tp), device_id_type=MESH)
    for dy in range(SIDE):
        for dx in range(SIDE):
            if dy or dx:
                pl.semaphore_signal(barrier, inc=1, device_id=(ep, tp_of(0, dx, dy)), device_id_type=MESH)

    for load in small:
        load.wait()

    def tables(shape, dim):
        r = iota(shape, dim)
        j = lax.shift_right_logical(r * (65536 // cap + 1), 16)
        e = lax.bitwise_and(z + lax.shift_right_logical(j, 1), zs - 1) * 2 + lax.bitwise_and(c + j, 1)
        return e, (r - cap * j).astype(F32)

    def flag(m):
        return jnp.where(m, 1.0, 0.0).astype(BF)

    def weight(x):
        return x.astype(BF).astype(F32)

    before = flag(iota((n_tok, n_tok), 0) < iota((n_tok, n_tok), 1))
    after = flag(iota((n_tok, n_tok), 0) > iota((n_tok, n_tok), 1))
    e, s = tables((rows, n_tok), 0)
    first = routes_t[0:1, :] == e
    hit = first | (routes_t[1:2, :] == e)
    chosen = hit & (dot(flag(hit), before, 1, 0) == s)
    wt = weight(rw_t[...])
    slot_w = jnp.sum(jnp.where(chosen, jnp.where(first, wt[0:1, :], wt[1:2, :]), 0.0), axis=1, keepdims=True)
    pick = flag(chosen)
    sbv = sb.reshape(4, rows, 128)
    for g in range(2):
        sbv[g] = dot(pick, tok[:, g * 128 : (g + 1) * 128], 1, 0).astype(BF)
        sbv[2 + g] = (slot_w * dot(pick, og[:, g * 128 : (g + 1) * 128], 1, 0)).astype(BF)

    share = sg_o.shape[0]
    for b in range(sp.shape[0]):
        for cc in range(2):
            lo = (b * 2 + cc) * share
            if lo % 128 == 0:
                wide = dot(sh[:, lo : lo + 128], og[...], 0, 0)
            sp[b, cc] = wide[lo % 128 : lo % 128 + share]

    pl.semaphore_wait(barrier, slots - 1 + n_tp - 1)

    def slot_in(d, cd):
        return [g.index(d) for g in groups if d in g][0] * 2 + cd

    def exchange(chunk):
        for d in groups[chunk]:
            for cd in (1, 0):
                if d or cd:
                    j = (d % zs) * 2 + cd
                    remote(
                        sb.at[:, pl.ds(j * pairs, pairs)],
                        xa.at[chunk, tp, :, pl.ds(slot_in(d, cd) * pairs, pairs)],
                        z_send, z_recv.at[chunk], (ep_of(d, cd), tp),
                    ).start()

    for ch in range(nch):
        exchange(ch)
    xa[0, tp, :, pl.ds(slot_in(0, 0) * pairs, pairs)] = sb[:, pl.ds(0, pairs)]

    remote(sp.at[:, 1 - c], sc, sc_send, sc_recv, (ep_of(0, 1), tp)).start()

    def term(d):
        zz = ring(d)
        return sp[zz, c] + sc[zz]

    far = zs // 2

    def shared(step):
        if step == 0:
            arrived(sc, sc_recv)
        for way, hops in ((0, far), (1, far - 1)):
            sign = 1 if way == 0 else -1
            if step > hops:
                continue
            total = term(sign * (hops - step))
            if step:
                arrived(shb.at[way, step - 1], sh_recv.at[way, step - 1])
                total = total + shb[way, step - 1]
            if step < hops:
                shs[way, step] = total
                remote(
                    shs.at[way, step], shb.at[way, step], sh_send.at[way, step], sh_recv.at[way, step],
                    (ep_of(sign, 0), tp),
                ).start()
            elif way == 1:
                sg_o[...] = total
            else:
                sg_o[...] = sg_o[...] + total - term(0)

    back = (0, -1, 1, 2)

    def gather_send(ch, h, k, kind, t, g0, gn, dev_t):
        ref = xa.at[ch, t, pl.ds(2 * h + g0, gn)]
        remote(ref, ref, ag_send, ag_recv.at[ch, h, k, kind], (ep, dev_t)).start()

    def gather_wait(ch, h, k, kind, g0, gn):
        arrived(xa.at[ch, 0, pl.ds(2 * h + g0, gn)], ag_recv.at[ch, h, k, kind])

    def spread(ch, h, k):
        t = tp_of(h, back[k], 0)
        gather_send(ch, h, k, 0, t, 0, 2, tp_of(h, 0, 1))
        gather_send(ch, h, k, 1, t, 0, 2, tp_of(h, 0, -1))

    def relay(ch, h, k):
        gather_wait(ch, h, k, 0, 0, 2)
        gather_send(ch, h, k, 2, tp_of(h, back[k], -1), 0, 1, tp_of(h, 0, 1))
        gather_wait(ch, h, k, 1, 0, 2)
        gather_send(ch, h, k, 3, tp_of(h, back[k], 1), 1, 1, tp_of(h, 0, -1))

    def g_0(ch):
        arrived(xa.at[ch, 0, :, pl.ds(0, (ns - (1 if ch == 0 else 0)) * pairs)], z_recv.at[ch])
        for h in range(2):
            gather_send(ch, h, 4, 0, tp, 0, 2, tp_of(h, 1, 0))
            gather_send(ch, h, 4, 1, tp, 0, 2, tp_of(h, -1, 0))
        for h in range(2):
            spread(ch, h, 0)

    def g_1(ch):
        for h in range(2):
            gather_wait(ch, h, 4, 0, 0, 2)
            gather_send(ch, h, 4, 2, tp_of(h, -1, 0), 0, 1, tp_of(h, 1, 0))
            gather_wait(ch, h, 4, 1, 0, 2)
            gather_send(ch, h, 4, 3, tp_of(h, 1, 0), 1, 1, tp_of(h, -1, 0))
        for h in range(2):
            spread(ch, h, 1)
            spread(ch, h, 2)

    def g_2(ch):
        for h in range(2):
            relay(ch, h, 0)
        for h in range(2):
            gather_wait(ch, h, 4, 2, 0, 1)
            gather_wait(ch, h, 4, 3, 1, 1)
            spread(ch, h, 3)

    def g_3(ch):
        for h in range(2):
            relay(ch, h, 1)
            relay(ch, h, 2)

    def g_4(ch):
        for h in range(2):
            relay(ch, h, 3)

    def g_5(ch):
        for h in range(2):
            for k in range(4):
                gather_wait(ch, h, k, 2, 0, 1)
                gather_wait(ch, h, k, 3, 1, 1)

    xav = xa.reshape(nch, n_tp, 4, half, 128)
    width = 256

    def expert(ch):
        def sums(i, total):
            a, b = total
            for u in range(4):
                t = i * 4 + u
                cols = pl.ds(pl.multiple_of(t * width, width), width)
                x = jnp.concatenate([xav[ch, t, 0], xav[ch, t, 1]], axis=1)
                y = jnp.concatenate([xav[ch, t, 2], xav[ch, t, 3]], axis=1)
                a = a + dot(x, wgu[:, cols], 1, 1)
                b = b + dot(y, wdn[:, cols], 1, 1)
            return a, b

        start = (jnp.zeros((half, 2 * fe), F32), jnp.zeros((half, fe), F32))
        gu, back_grad = lax.fori_loop(0, n_tp // 4, sums, start)
        pre_gate, pre_up = gu[:, :fe], gu[:, fe:]
        squash = 1.0 / (1.0 + jnp.exp(-pre_gate))
        activated = pre_gate * squash
        hidden = (activated * pre_up).astype(BF)
        gate_delta = back_grad * pre_up * squash * (1.0 + pre_gate * (1.0 - squash))
        at = pl.ds(ch * half, half)
        deltas = jnp.concatenate([gate_delta, back_grad * activated], axis=1)
        dl[at, :] = deltas.astype(BF)
        hd[at, :] = hidden
        product = hidden.astype(F32) * back_grad
        line = dot(jnp.ones((8, fe), F32), product, 1, 1, HIGH)
        pb[tp, pl.ds(ch, 1), pl.ds(0, half)] = line[0:1]

    def parts(ch):
        at = pl.ds(ch * half, half)
        for dy in range(SIDE):
            for dx in range(SIDE):
                t = tp_of(0, dx, dy)
                cols = pl.ds(pl.multiple_of(t * width, width), width)
                out = dot(dl[at, :], wgu[:, cols], 1, 0).astype(BF)
                pr[ch, 0, dx, dy] = out[:, :128]
                pr[ch, 1, dy, dx] = out[:, 128:]

    def add(*xs):
        total = xs[0].astype(F32)
        for x in xs[1:]:
            total = total + x.astype(F32)
        return total

    def landing(ch, h, i, base):
        if base == 0:
            return r1.at[ch, h, i], 0
        if i in (0, 3, 4):
            return r2t.at[ch, h, (0, 3, 4).index(i)], 1
        return r2l.at[ch, h, (1, 2, 5).index(i)], 2

    def sum_send(ch, h, src, i, base, dev_t):
        dst, kind = landing(ch, h, i, base)
        remote(src, dst, rs_send.at[kind], rs_recv.at[ch, h, base + i], (ep, dev_t)).start()

    def sum_wait(ch, h, i, base):
        arrived(landing(ch, h, i, base)[0], rs_recv.at[ch, h, base + i])

    lo, hi = pl.ds(0, 2), pl.ds(2, 2)
    top, low = pl.ds(0, cut), pl.ds(cut, half - cut)

    def q_0(ch):
        for h in range(2):
            sum_send(ch, h, pr.at[ch, h, 2, lo], 0, 0, tp_of(h, 1, 0))
            sum_send(ch, h, pr.at[ch, h, 2, hi], 1, 0, tp_of(h, -1, 0))
        for h in range(2):
            sum_send(ch, h, pr.at[ch, h, 1, hi], 2, 0, tp_of(h, 1, 0))
            sum_send(ch, h, pr.at[ch, h, 3, lo], 3, 0, tp_of(h, -1, 0))

    def q_1(ch):
        for h in range(2):
            sum_wait(ch, h, 0, 0)
            f1[ch, h, 0] = add(pr[ch, h, 1, lo], r1[ch, h, 0]).astype(BF)
            sum_send(ch, h, f1.at[ch, h, 0], 4, 0, tp_of(h, 1, 0))
            sum_wait(ch, h, 1, 0)
            f1[ch, h, 1] = add(pr[ch, h, 3, hi], r1[ch, h, 1]).astype(BF)
            sum_send(ch, h, f1.at[ch, h, 1], 5, 0, tp_of(h, -1, 0))

    def q_2(ch):
        for h in range(2):
            for i in (3, 2, 4, 5):
                sum_wait(ch, h, i, 0)
            for ds in (2, 1, 3, 0):
                pair = (4, 3) if ds < 2 else (2, 5)
                total = add(pr[ch, h, 0, ds], r1[ch, h, pair[0], ds % 2], r1[ch, h, pair[1], ds % 2])
                if ds:
                    s1[ch, h, ds - 1] = total.astype(BF)
                else:
                    s0[ch, h] = total
            sum_send(ch, h, s1.at[ch, h, 1, top], 0, 6, tp_of(h, 0, 1))
            sum_send(ch, h, s1.at[ch, h, 1, low], 1, 6, tp_of(h, 0, -1))
            sum_send(ch, h, s1.at[ch, h, 0, low], 2, 6, tp_of(h, 0, 1))
            sum_send(ch, h, s1.at[ch, h, 2, top], 3, 6, tp_of(h, 0, -1))

    def q_3(ch):
        for h in range(2):
            sum_wait(ch, h, 0, 6)
            f2t[ch, h] = add(s1[ch, h, 0, top], r2t[ch, h, 0]).astype(BF)
            sum_send(ch, h, f2t.at[ch, h], 4, 6, tp_of(h, 0, 1))
            sum_wait(ch, h, 1, 6)
            f2l[ch, h] = add(s1[ch, h, 2, low], r2l[ch, h, 0]).astype(BF)
            sum_send(ch, h, f2l.at[ch, h], 5, 6, tp_of(h, 0, -1))

    rtv = rt.reshape(nch, 2, half, 128)

    def q_4(ch):
        for h in range(2):
            for i in (3, 2, 4, 5):
                sum_wait(ch, h, i, 6)
            rtv[ch, h, top] = add(s0[ch, h, top], r2t[ch, h, 2], r2t[ch, h, 1]).astype(BF)
            rtv[ch, h, low] = add(s0[ch, h, low], r2l[ch, h, 1], r2l[ch, h, 2]).astype(BF)
        for d in groups[ch][::-1]:
            for cd in (1, 0):
                here = pl.ds(slot_in(d, cd) * pairs, pairs)
                there = pl.ds(((d % zs) * 2 + cd) * pairs, pairs)
                if d or cd:
                    remote(
                        rt.at[ch, :, here], rh.at[:, there], rz_send, rz_recv, (ep_of(-d, cd), tp)
                    ).start()
                else:
                    rh[:, there] = rt[ch, :, here]

    def product_send():
        for dy in range(SIDE):
            for dx in range(SIDE):
                if dy or dx:
                    remote(pb.at[tp], pb.at[tp], pb_send, pb_recv, (ep, tp_of(0, dx, dy))).start()

    def product_return():
        arrived(pb.at[pl.ds(0, n_tp - 1)], pb_recv)
        for ch in range(nch):
            total = pb[0, pl.ds(ch, 1), pl.ds(0, half)]
            for t in range(1, n_tp):
                total = total + pb[t, pl.ds(ch, 1), pl.ds(0, half)]
            r = iota((ns, half), 1)
            j = lax.shift_right_logical(r * (65536 // cap + 1), 16)
            own = jnp.where(j == iota((ns, half), 0), total, 0.0)
            r = iota((half, 128), 0)
            j = lax.shift_right_logical(r * (65536 // cap + 1), 16)
            lane = jnp.where(r - cap * j == iota((half, 128), 1), 1.0, 0.0)
            table = dot(own, lane, 1, 0, HIGH)
            for i in range(ns):
                pz[ch * ns + i] = table[i : i + 1]
        for ch in range(nch):
            for d in groups[ch][::-1]:
                for cd in (1, 0):
                    i, j = ch * ns + slot_in(d, cd), (d % zs) * 2 + cd
                    if d or cd:
                        remote(pz.at[i], ph.at[j], pz_send, pz_recv, (ep_of(-d, cd), tp)).start()
                    else:
                        ph[j] = pz[i]

    def weight_grads(t0, t1):
        def one(t, carry):
            cols = pl.ds(pl.multiple_of(t * width, width), width)
            both = jnp.zeros((2 * fe, width), F32)
            last = jnp.zeros((fe, width), F32)
            for ch in range(nch):
                x = jnp.concatenate([xav[ch, t, 0], xav[ch, t, 1]], axis=1)
                y = jnp.concatenate([xav[ch, t, 2], xav[ch, t, 3]], axis=1)
                both = both + dot(dlt[ch], x, 1, 0)
                last = last + dot(hdt[ch], y, 1, 0)
            gg_o[:, cols] = both[:fe].astype(BF)
            ug_o[:, cols] = both[fe:].astype(BF)
            dg_o[:, cols] = last.astype(BF)
            return carry

        lax.fori_loop(t0, t1, one, 0)

    def turned(ch):
        at = pl.ds(ch * half, half)
        dlt[ch] = dl[at, :].astype(F32).T.astype(BF)
        hdt[ch] = hd[at, :].astype(F32).T.astype(BF)

    shared(0)
    g_0(0)
    g_1(0)
    g_0(1)
    g_2(0)
    g_1(1)
    g_3(0)
    g_2(1)
    g_0(2)
    g_4(0)
    g_3(1)
    g_1(2)
    g_5(0)
    for load in loads:
        load.wait()
    expert(0)
    g_4(1)
    g_2(2)
    g_0(3)
    shared(1)
    g_5(1)
    g_3(2)
    parts(0)
    g_1(3)
    shared(2)
    expert(1)
    g_4(2)
    g_2(3)
    shared(3)
    parts(1)
    g_5(2)
    g_3(3)
    shared(4)
    q_0(0)
    expert(2)
    g_4(3)
    q_0(1)
    shared(5)
    q_1(0)
    parts(2)
    q_0(2)
    g_5(3)
    q_1(1)
    shared(6)
    expert(3)
    parts(3)
    q_0(3)
    product_send()
    q_2(0)
    q_1(2)
    shared(7)
    q_2(1)
    q_1(3)
    shared(8)
    q_3(0)
    turned(0)
    turned(1)
    q_2(2)
    q_3(1)
    q_4(0)
    q_2(3)
    turned(2)
    turned(3)
    q_3(2)
    q_4(1)
    weight_grads(0, 1)
    q_3(3)
    product_return()
    q_4(2)
    weight_grads(1, 2)
    q_4(3)
    weight_grads(2, 16)

    e, s = tables((n_tok, rows), 1)
    def turn(row):
        return jnp.broadcast_to(row, (n_tok, n_tok)).T

    r0, r1c = (turn(routes_t[k : k + 1, :].astype(F32))[:, 0:1].astype(jnp.int32) for k in range(2))
    hit = (r0 == e) | (r1c == e)
    cm[...] = flag(hit & (dot(after, flag(hit), 1, 0) == s))
    j = iota((n_tok, slots), 1)
    ej = lax.bitwise_and(z + lax.shift_right_logical(j, 1), zs - 1) * 2 + lax.bitwise_and(c + j, 1)
    seen = dot(after, flag((r0 == ej) | (r1c == ej)), 1, 0)
    arrived(ph.at[pl.ds(0, slots - 1)], pz_recv)
    table = jnp.concatenate([ph[i] for i in range(slots)], axis=0)
    for k in range(2):
        mine = (r0, r1c)[k] == ej
        rank = jnp.sum(jnp.where(mine, seen, 0.0), axis=1, keepdims=True)
        found = dot(jnp.where(mine, 1.0, 0.0), table, 1, 0, HIGH)
        lane = iota((n_tok, 128), 1).astype(F32)
        value = jnp.sum(jnp.where(lane == rank, found, 0.0), axis=1, keepdims=True)
        row = jnp.broadcast_to(value, (n_tok, n_tok)).T[0:1]
        wg_o[k : k + 1, :] = row / wt[k : k + 1, :]
    arrived(rh.at[:, pl.ds(0, (slots - 1) * pairs)], rz_recv)
    rhv = rh.reshape(2, rows, 128)
    for h in range(2):
        tg_o[:, h * 128 : (h + 1) * 128] = dot(cm[...], rhv[h], 1, 0).astype(BF)

    left(sb.at[:, pl.ds(0, (slots - 1) * pairs)], z_send)
    left(xa.at[:, pl.ds(0, n_tp - 1)], ag_send)
    left(r1, rs_send.at[0])
    left(r2t, rs_send.at[1])
    left(r2l, rs_send.at[2])
    left(rh.at[:, pl.ds(0, (slots - 1) * pairs)], rz_send)
    left(pb.at[pl.ds(0, n_tp - 1)], pb_send)
    left(ph.at[pl.ds(0, slots - 1)], pz_send)
    left(sc, sc_send)
    for way, hops in ((0, far), (1, far - 1)):
        for step in range(hops):
            left(shs.at[way, step], sh_send.at[way, step])


def settle(*refs):
    n = len(refs) // 3
    src, dst, held, sems = refs[:n], refs[n : 2 * n], refs[2 * n : 3 * n], refs[3 * n :]
    into = [pltpu.make_async_copy(src[i], held[i], sems[0].at[i]) for i in range(n)]
    out = [pltpu.make_async_copy(held[i], dst[i], sems[1].at[i]) for i in range(n)]
    for copy in into:
        copy.start()
    for i in range(n):
        into[i].wait()
        out[i].start()
    for copy in out:
        copy.wait()


def local(zs, tokens, out_grad, routes, route_weights, gate_proj, up_proj, down_proj, shared_hidden):
    n_tok, feat = tokens.shape
    _, fe, width = gate_proj.shape
    slots = 2 * zs
    cap = max(2, 5 * n_tok * routes.shape[1] // (4 * slots))
    rows = slots * cap
    nch = len(chunks_of(zs))
    half = rows // nch
    cut = (half // 2 + 15) // 16 * 16
    n_tp = SIDE * SIDE
    share = shared_hidden.shape[1] // slots
    far = zs // 2
    vmem = pl.BlockSpec(memory_space=pltpu.VMEM)
    hbm = pl.BlockSpec(memory_space=pltpu.HBM)
    dma = pltpu.SemaphoreType.DMA
    V = pltpu.VMEM
    out = pl.pallas_call(
        functools.partial(kernel, zs, cap),
        out_shape=(
            jax.ShapeDtypeStruct((n_tok, feat), BF),
            jax.ShapeDtypeStruct((2, n_tok), F32),
            jax.ShapeDtypeStruct((fe, width), BF),
            jax.ShapeDtypeStruct((fe, width), BF),
            jax.ShapeDtypeStruct((fe, width), BF),
            jax.ShapeDtypeStruct((share, feat), F32),
        ),
        in_specs=[hbm] * 8,
        out_specs=(vmem,) * 6,
        scratch_shapes=[
            V((n_tok, feat), BF),
            V((n_tok, feat), BF),
            V((2, n_tok), jnp.int32),
            V((2, n_tok), F32),
            V(shared_hidden.shape, BF),
            V((2 * fe, width), BF),
            V((fe, width), BF),
            V((4, rows // 2, 2, 128), BF),
            V((nch, n_tp, 4, half // 2, 2, 128), BF),
            V((rows, 2 * fe), BF),
            V((rows, fe), BF),
            V((nch, 2 * fe, half), BF),
            V((nch, fe, half), BF),
            V((nch, 2, SIDE, SIDE, half, 128), BF),
            V((nch, 2, 6, 2, half, 128), BF),
            V((nch, 2, 2, 2, half, 128), BF),
            V((nch, 2, half, 128), F32),
            V((nch, 2, 3, half, 128), BF),
            V((nch, 2, 3, cut, 128), BF),
            V((nch, 2, 3, half - cut, 128), BF),
            V((nch, 2, cut, 128), BF),
            V((nch, 2, half - cut, 128), BF),
            V((nch, 2, half // 2, 2, 128), BF),
            V((2, rows // 2, 2, 128), BF),
            V((n_tp, nch, (half + 127) // 128 * 128), F32),
            V((slots, 1, 128), F32),
            V((slots, 1, 128), F32),
            V((n_tok, rows), BF),
            V((zs, 2, share, feat), F32),
            V((zs, share, feat), F32),
            V((2, far, share, feat), F32),
            V((2, far, share, feat), F32),
            dma((8,)),
            dma, dma((nch,)),
            dma, dma((nch, 2, 5, 4)),
            dma((3,)), dma((nch, 2, 12)),
            dma, dma,
            dma, dma,
            dma, dma,
            dma, dma,
            dma((2, far)), dma((2, far)),
        ],
        compiler_params=pltpu.CompilerParams(collective_id=0, has_side_effects=True, vmem_limit_bytes=60 * 1024 * 1024),
    )(
        tokens, out_grad, routes.T, route_weights.T,
        gate_proj[0], up_proj[0], down_proj[0], shared_hidden,
    )
    shapes = [jax.ShapeDtypeStruct(a.shape, a.dtype) for a in out]
    tg, wg, gg, ug, dg, sg = pl.pallas_call(
        settle,
        out_shape=shapes,
        in_specs=[hbm] * len(out),
        out_specs=[hbm] * len(out),
        scratch_shapes=[V(a.shape, a.dtype) for a in out] + [dma((len(out),)), dma((len(out),))],
    )(*out)
    return tg, wg.T, gg[None], ug[None], dg[None], sg


def solution(mesh):
    zs = mesh.shape["ep"] // 2
    features, whole, weights = P("ep", "tp"), P("ep", None), P("ep", "tp", None)
    return jax.shard_map(
        functools.partial(local, zs),
        mesh=mesh,
        in_specs=(features, features, whole, whole, weights, weights, weights, whole),
        out_specs=(features, whole, weights, weights, weights, features),
        check_vma=False,
    )
```

```python
import functools

import jax
import jax.numpy as jnp
from jax import lax
from jax.experimental import pallas as pl
from jax.experimental.pallas import tpu as pltpu
from jax.sharding import PartitionSpec as P

MESH = pl.DeviceIdType.MESH
BF = jnp.bfloat16
F32 = jnp.float32
SIDE = 4
ORDER = (0, 3, 2, 1)
HIGH = lax.Precision.HIGHEST


def chunks_of(zs):
    near = sorted(range(1 - zs // 2, zs // 2 + 1), key=lambda d: (abs(d), -d))
    size = zs // len(ORDER)
    parts = [near[k * size : (k + 1) * size] for k in range(len(ORDER))]
    return [parts[k] for k in ORDER]


def dot(a, b, da, db, precision=None):
    return lax.dot_general(
        a, b, (((da,), (db,)), ((), ())), preferred_element_type=F32, precision=precision
    )


def iota(shape, dim):
    return lax.broadcasted_iota(jnp.int32, shape, dim)


def kernel(
    zs, cap,
    tok_h, og_h, routes_h, rw_h, gate, up, down, sh_h,
    tg_o, wg_o, gg_o, ug_o, dg_o, sg_o,
    tok, og, routes_t, rw_t, sh, wgu, wdn, sb, xa, dl, hd, dlt, hdt, pr, r1, f1, s0, s1, r2, rt, rh, pb, pz, ph, cm,
    sp, sc, shb, shs, ea, eb,
    w_sem, z_send, z_recv, ag_send, ag_recv, rs_send, rs_recv, rz_send, rz_recv,
    pb_send, pb_recv, pz_send, pz_recv, sc_send, sc_recv, sh_send, sh_recv,
):
    ep, tp = lax.axis_index("ep"), lax.axis_index("tp")
    z, c = ep // 2, lax.rem(ep, 2)
    yx = (tp // SIDE, lax.rem(tp, SIDE))
    n_tp = SIDE * SIDE
    slots = 2 * zs
    rows = slots * cap
    groups = chunks_of(zs)
    nch = len(groups)
    ns = slots // nch
    half = rows // nch
    pairs = cap // 2
    fe = gate.shape[0]
    n_tok = tok.shape[0]

    def ring(d):
        return lax.rem(z + d + zs, zs)

    def ep_of(d, cd):
        return ring(d) * 2 + lax.rem(c + cd, 2)

    def tp_of(h, dp, ds):
        dy, dx = (ds, dp) if h == 0 else (dp, ds)
        return lax.rem(yx[0] + dy + SIDE, SIDE) * SIDE + lax.rem(yx[1] + dx + SIDE, SIDE)

    def remote(src, dst, ssem, rsem, dev):
        return pltpu.make_async_remote_copy(
            src_ref=src, dst_ref=dst, send_sem=ssem, recv_sem=rsem,
            device_id=dev, device_id_type=MESH,
        )

    def arrived(ref, sem):
        remote(ref, ref, sem, sem, (ep, tp)).wait_recv()

    def left(ref, sem):
        remote(ref, ref, sem, sem, (ep, tp)).wait_send()

    loads = [
        pltpu.make_async_copy(gate, wgu.at[pl.ds(0, fe)], w_sem.at[0]),
        pltpu.make_async_copy(up, wgu.at[pl.ds(fe, fe)], w_sem.at[1]),
        pltpu.make_async_copy(down, wdn, w_sem.at[2]),
    ]
    small = [
        pltpu.make_async_copy(src, dst, w_sem.at[3 + i])
        for i, (src, dst) in enumerate(
            ((routes_h, routes_t), (rw_h, rw_t), (tok_h, tok), (og_h, og), (sh_h, sh))
        )
    ]
    for load in small + loads:
        load.start()

    barrier = pltpu.get_barrier_semaphore()
    for d in range(zs):
        for cd in range(2):
            if d or cd:
                pl.semaphore_signal(barrier, inc=1, device_id=(ep_of(d, cd), tp), device_id_type=MESH)
    for dy in range(SIDE):
        for dx in range(SIDE):
            if dy or dx:
                pl.semaphore_signal(barrier, inc=1, device_id=(ep, tp_of(0, dx, dy)), device_id_type=MESH)

    for load in small:
        load.wait()

    def tables(shape, dim):
        r = iota(shape, dim)
        j = lax.shift_right_logical(r * (65536 // cap + 1), 16)
        e = lax.bitwise_and(z + lax.shift_right_logical(j, 1), zs - 1) * 2 + lax.bitwise_and(c + j, 1)
        return e, (r - cap * j).astype(F32)

    def flag(m):
        return jnp.where(m, 1.0, 0.0).astype(BF)

    def weight(x):
        return x.astype(BF).astype(F32)

    before = flag(iota((n_tok, n_tok), 0) < iota((n_tok, n_tok), 1))
    after = flag(iota((n_tok, n_tok), 0) > iota((n_tok, n_tok), 1))
    e, s = tables((rows, n_tok), 0)
    first = routes_t[0:1, :] == e
    hit = first | (routes_t[1:2, :] == e)
    chosen = hit & (dot(flag(hit), before, 1, 0) == s)
    wt = weight(rw_t[...])
    slot_w = jnp.sum(jnp.where(chosen, jnp.where(first, wt[0:1, :], wt[1:2, :]), 0.0), axis=1, keepdims=True)
    pick = flag(chosen)
    sbv = sb.reshape(4, rows, 128)
    for g in range(2):
        sbv[g] = dot(pick, tok[:, g * 128 : (g + 1) * 128], 1, 0).astype(BF)
        sbv[2 + g] = (slot_w * dot(pick, og[:, g * 128 : (g + 1) * 128], 1, 0)).astype(BF)

    share = sg_o.shape[0]
    for b in range(sp.shape[0]):
        for cc in range(2):
            lo = (b * 2 + cc) * share
            if lo % 128 == 0:
                wide = dot(sh[:, lo : lo + 128], og[...], 0, 0)
            sp[b, cc] = wide[lo % 128 : lo % 128 + share]

    pl.semaphore_wait(barrier, slots - 1 + n_tp - 1)

    def slot_in(d, cd):
        return [g.index(d) for g in groups if d in g][0] * 2 + cd

    def exchange(chunk):
        for d in groups[chunk]:
            for cd in (1, 0):
                if d or cd:
                    j = (d % zs) * 2 + cd
                    remote(
                        sb.at[:, pl.ds(j * pairs, pairs)],
                        xa.at[chunk, tp, :, pl.ds(slot_in(d, cd) * pairs, pairs)],
                        z_send, z_recv.at[chunk], (ep_of(d, cd), tp),
                    ).start()

    for ch in range(nch):
        exchange(ch)
    xa[0, tp, :, pl.ds(slot_in(0, 0) * pairs, pairs)] = sb[:, pl.ds(0, pairs)]

    remote(sp.at[:, 1 - c], sc, sc_send, sc_recv, (ep_of(0, 1), tp)).start()

    def term(d):
        zz = ring(d)
        return sp[zz, c] + sc[zz]

    far = zs // 2

    def shared(step):
        if step == 0:
            arrived(sc, sc_recv)
        for way, hops in ((0, far), (1, far - 1)):
            sign = 1 if way == 0 else -1
            if step > hops:
                continue
            total = term(sign * (hops - step))
            if step:
                arrived(shb.at[way, step - 1], sh_recv.at[way, step - 1])
                total = total + shb[way, step - 1]
            if step < hops:
                shs[way, step] = total
                remote(
                    shs.at[way, step], shb.at[way, step], sh_send.at[way, step], sh_recv.at[way, step],
                    (ep_of(sign, 0), tp),
                ).start()
            elif way == 1:
                sg_o[...] = total
            else:
                sg_o[...] = sg_o[...] + total - term(0)

    back = (0, -1, 1, 2)

    def gather_send(ch, h, k, kind, t, g0, gn, dev_t):
        ref = xa.at[ch, t, pl.ds(2 * h + g0, gn)]
        remote(ref, ref, ag_send, ag_recv.at[ch, h, k, kind], (ep, dev_t)).start()

    def gather_wait(ch, h, k, kind, g0, gn):
        arrived(xa.at[ch, 0, pl.ds(2 * h + g0, gn)], ag_recv.at[ch, h, k, kind])

    def spread(ch, h, k):
        t = tp_of(h, back[k], 0)
        gather_send(ch, h, k, 0, t, 0, 2, tp_of(h, 0, 1))
        gather_send(ch, h, k, 1, t, 0, 2, tp_of(h, 0, -1))

    def relay(ch, h, k):
        gather_wait(ch, h, k, 0, 0, 2)
        gather_send(ch, h, k, 2, tp_of(h, back[k], -1), 0, 1, tp_of(h, 0, 1))
        gather_wait(ch, h, k, 1, 0, 2)
        gather_send(ch, h, k, 3, tp_of(h, back[k], 1), 1, 1, tp_of(h, 0, -1))

    def g_0(ch):
        arrived(xa.at[ch, 0, :, pl.ds(0, (ns - (1 if ch == 0 else 0)) * pairs)], z_recv.at[ch])
        for h in range(2):
            gather_send(ch, h, 4, 0, tp, 0, 2, tp_of(h, 1, 0))
            gather_send(ch, h, 4, 1, tp, 0, 2, tp_of(h, -1, 0))
        for h in range(2):
            spread(ch, h, 0)

    def g_1(ch):
        for h in range(2):
            gather_wait(ch, h, 4, 0, 0, 2)
            gather_send(ch, h, 4, 2, tp_of(h, -1, 0), 0, 1, tp_of(h, 1, 0))
            gather_wait(ch, h, 4, 1, 0, 2)
            gather_send(ch, h, 4, 3, tp_of(h, 1, 0), 1, 1, tp_of(h, -1, 0))
        for h in range(2):
            spread(ch, h, 1)
            spread(ch, h, 2)

    def g_2(ch):
        for h in range(2):
            relay(ch, h, 0)
        for h in range(2):
            gather_wait(ch, h, 4, 2, 0, 1)
            gather_wait(ch, h, 4, 3, 1, 1)
            spread(ch, h, 3)

    def g_3(ch):
        for h in range(2):
            relay(ch, h, 1)
            relay(ch, h, 2)

    def g_4(ch):
        for h in range(2):
            relay(ch, h, 3)

    def g_5(ch, ks=range(4)):
        for h in range(2):
            for k in ks:
                gather_wait(ch, h, k, 2, 0, 1)
                gather_wait(ch, h, k, 3, 1, 1)

    xav = xa.reshape(nch, n_tp, 4, half, 128)
    width = 256

    def early(ch, dps, start):
        a, b = start
        for dp in dps:
            for ds in range(SIDE):
                t, u = tp_of(0, dp, ds), tp_of(1, dp, ds)
                x = jnp.concatenate([xav[ch, t, 0], xav[ch, t, 1]], axis=1)
                y = jnp.concatenate([xav[ch, u, 2], xav[ch, u, 3]], axis=1)
                a = a + dot(x, wgu[:, pl.ds(pl.multiple_of(t * width, width), width)], 1, 1)
                b = b + dot(y, wdn[:, pl.ds(pl.multiple_of(u * width, width), width)], 1, 1)
        return a, b

    def expert_early(ch):
        start = (jnp.zeros((half, 2 * fe), F32), jnp.zeros((half, fe), F32))
        ea[...], eb[...] = early(ch, (0, -1, 1), start)

    def expert(ch, late=False):
        def sums(i, total):
            a, b = total
            for u in range(4):
                t = i * 4 + u
                cols = pl.ds(pl.multiple_of(t * width, width), width)
                x = jnp.concatenate([xav[ch, t, 0], xav[ch, t, 1]], axis=1)
                y = jnp.concatenate([xav[ch, t, 2], xav[ch, t, 3]], axis=1)
                a = a + dot(x, wgu[:, cols], 1, 1)
                b = b + dot(y, wdn[:, cols], 1, 1)
            return a, b

        start = (jnp.zeros((half, 2 * fe), F32), jnp.zeros((half, fe), F32))
        if late:
            gu, back_grad = early(ch, (2,), (ea[...], eb[...]))
        else:
            gu, back_grad = lax.fori_loop(0, n_tp // 4, sums, start)
        pre_gate, pre_up = gu[:, :fe], gu[:, fe:]
        squash = 1.0 / (1.0 + jnp.exp(-pre_gate))
        activated = pre_gate * squash
        hidden = (activated * pre_up).astype(BF)
        gate_delta = back_grad * pre_up * squash * (1.0 + pre_gate * (1.0 - squash))
        at = pl.ds(ch * half, half)
        deltas = jnp.concatenate([gate_delta, back_grad * activated], axis=1)
        dl[at, :] = deltas.astype(BF)
        hd[at, :] = hidden
        product = hidden.astype(F32) * back_grad
        line = dot(jnp.ones((8, fe), F32), product, 1, 1, HIGH)
        pb[tp, pl.ds(ch, 1), pl.ds(0, half)] = line[0:1]

    def parts(ch, which=(True, False)):
        at = pl.ds(ch * half, half)
        for dy in range(SIDE):
            for dx in range(SIDE):
                if (2 in (dx, dy)) not in which:
                    continue
                t = tp_of(0, dx, dy)
                cols = pl.ds(pl.multiple_of(t * width, width), width)
                out = dot(dl[at, :], wgu[:, cols], 1, 0).astype(BF)
                pr[ch, 0, dx, dy] = out[:, :128]
                pr[ch, 1, dy, dx] = out[:, 128:]

    def add(*xs):
        total = xs[0].astype(F32)
        for x in xs[1:]:
            total = total + x.astype(F32)
        return total

    def landing(ch, h, i, base):
        return (r1 if base == 0 else r2).at[ch, h, i]

    def sum_send(ch, h, src, i, base, dev_t):
        remote(src, landing(ch, h, i, base), rs_send.at[base // 6], rs_recv.at[ch, h, base + i], (ep, dev_t)).start()

    def sum_wait(ch, h, i, base):
        arrived(landing(ch, h, i, base), rs_recv.at[ch, h, base + i])

    lo, hi = pl.ds(0, 2), pl.ds(2, 2)

    def q_0(ch):
        q_0a(ch)
        q_0b(ch)

    def q_0a(ch):
        for h in range(2):
            sum_send(ch, h, pr.at[ch, h, 2, lo], 0, 0, tp_of(h, 1, 0))
            sum_send(ch, h, pr.at[ch, h, 2, hi], 1, 0, tp_of(h, -1, 0))

    def q_0b(ch):
        for h in range(2):
            sum_send(ch, h, pr.at[ch, h, 1, hi], 2, 0, tp_of(h, 1, 0))
            sum_send(ch, h, pr.at[ch, h, 3, lo], 3, 0, tp_of(h, -1, 0))

    def q_1(ch):
        for h in range(2):
            sum_wait(ch, h, 0, 0)
            f1[ch, h, 0] = add(pr[ch, h, 1, lo], r1[ch, h, 0]).astype(BF)
            sum_send(ch, h, f1.at[ch, h, 0], 4, 0, tp_of(h, 1, 0))
            sum_wait(ch, h, 1, 0)
            f1[ch, h, 1] = add(pr[ch, h, 3, hi], r1[ch, h, 1]).astype(BF)
            sum_send(ch, h, f1.at[ch, h, 1], 5, 0, tp_of(h, -1, 0))

    def q_2(ch):
        for h in range(2):
            for i in (3, 2, 4, 5):
                sum_wait(ch, h, i, 0)
            for ds in (2, 1, 3, 0):
                pair = (4, 3) if ds < 2 else (2, 5)
                total = add(pr[ch, h, 0, ds], r1[ch, h, pair[0], ds % 2], r1[ch, h, pair[1], ds % 2])
                if ds:
                    s1[ch, h, ds - 1] = total.astype(BF)
                else:
                    s0[ch, h] = total
            for i, ds in ((1, 2), (0, 1), (2, -1)):
                sum_send(ch, h, s1.at[ch, h, i], i, 6, tp_of(h, 0, ds))

    rtv = rt.reshape(nch, 2, half, 128)

    def q_4(ch):
        for h in range(2):
            for i in (0, 2, 1):
                sum_wait(ch, h, i, 6)
            rtv[ch, h] = add(s0[ch, h], r2[ch, h, 0], r2[ch, h, 2], r2[ch, h, 1]).astype(BF)
        for d in groups[ch][::-1]:
            for cd in (1, 0):
                here = pl.ds(slot_in(d, cd) * pairs, pairs)
                there = pl.ds(((d % zs) * 2 + cd) * pairs, pairs)
                if d or cd:
                    remote(
                        rt.at[ch, :, here], rh.at[:, there], rz_send, rz_recv, (ep_of(-d, cd), tp)
                    ).start()
                else:
                    rh[:, there] = rt[ch, :, here]

    def product_send():
        for dy in range(SIDE):
            for dx in range(SIDE):
                if dy or dx:
                    remote(pb.at[tp], pb.at[tp], pb_send, pb_recv, (ep, tp_of(0, dx, dy))).start()

    def product_return():
        arrived(pb.at[pl.ds(0, n_tp - 1)], pb_recv)
        for ch in range(nch):
            total = pb[0, pl.ds(ch, 1), pl.ds(0, half)]
            for t in range(1, n_tp):
                total = total + pb[t, pl.ds(ch, 1), pl.ds(0, half)]
            r = iota((ns, half), 1)
            j = lax.shift_right_logical(r * (65536 // cap + 1), 16)
            own = jnp.where(j == iota((ns, half), 0), total, 0.0)
            r = iota((half, 128), 0)
            j = lax.shift_right_logical(r * (65536 // cap + 1), 16)
            lane = jnp.where(r - cap * j == iota((half, 128), 1), 1.0, 0.0)
            table = dot(own, lane, 1, 0, HIGH)
            for i in range(ns):
                pz[ch * ns + i] = table[i : i + 1]
        for ch in range(nch):
            for d in groups[ch][::-1]:
                for cd in (1, 0):
                    i, j = ch * ns + slot_in(d, cd), (d % zs) * 2 + cd
                    if d or cd:
                        remote(pz.at[i], ph.at[j], pz_send, pz_recv, (ep_of(-d, cd), tp)).start()
                    else:
                        ph[j] = pz[i]

    def weight_grads(t0, t1):
        def one(t, carry):
            cols = pl.ds(pl.multiple_of(t * width, width), width)
            both = jnp.zeros((2 * fe, width), F32)
            last = jnp.zeros((fe, width), F32)
            for ch in range(nch):
                x = jnp.concatenate([xav[ch, t, 0], xav[ch, t, 1]], axis=1)
                y = jnp.concatenate([xav[ch, t, 2], xav[ch, t, 3]], axis=1)
                both = both + dot(dlt[ch], x, 1, 0)
                last = last + dot(hdt[ch], y, 1, 0)
            gg_o[:, cols] = both[:fe].astype(BF)
            ug_o[:, cols] = both[fe:].astype(BF)
            dg_o[:, cols] = last.astype(BF)
            return carry

        lax.fori_loop(t0, t1, one, 0)

    def turned(ch):
        at = pl.ds(ch * half, half)
        dlt[ch] = dl[at, :].astype(F32).T.astype(BF)
        hdt[ch] = hd[at, :].astype(F32).T.astype(BF)

    shared(0)
    g_0(0)
    g_1(0)
    g_2(0)
    g_0(1)
    g_3(0)
    g_1(1)
    g_0(2)
    g_4(0)
    g_0(3)
    shared(1)
    g_2(1)
    g_1(2)
    g_5(0)
    for load in loads:
        load.wait()
    expert(0)
    shared(2)
    g_1(3)
    g_3(1)
    g_2(2)
    shared(3)
    parts(0)
    g_4(1)
    g_2(3)
    g_3(2)
    shared(4)
    g_5(1)
    g_3(3)
    g_4(2)
    expert(1)
    shared(5)
    g_4(3)
    q_0(0)
    parts(1)
    q_0(1)
    g_5(2)
    shared(6)
    expert(2)
    q_1(0)
    parts(2)
    q_0(2)
    q_1(1)
    g_5(3, (0, 1, 2))
    shared(7)
    expert_early(3)
    g_5(3, (3,))
    expert(3, True)
    parts(3, (True,))
    q_0a(3)
    parts(3, (False,))
    q_0b(3)
    product_send()
    q_2(0)
    q_1(2)
    q_2(1)
    q_1(3)
    shared(8)
    q_4(0)
    turned(0)
    turned(1)
    q_2(2)
    q_4(1)
    q_2(3)
    turned(2)
    turned(3)
    weight_grads(0, 1)
    product_return()
    q_4(2)
    weight_grads(1, 2)
    q_4(3)
    weight_grads(2, 16)

    e, s = tables((n_tok, rows), 1)
    def turn(row):
        return jnp.broadcast_to(row, (n_tok, n_tok)).T

    r0, r1c = (turn(routes_t[k : k + 1, :].astype(F32))[:, 0:1].astype(jnp.int32) for k in range(2))
    hit = (r0 == e) | (r1c == e)
    cm[...] = flag(hit & (dot(after, flag(hit), 1, 0) == s))
    j = iota((n_tok, slots), 1)
    ej = lax.bitwise_and(z + lax.shift_right_logical(j, 1), zs - 1) * 2 + lax.bitwise_and(c + j, 1)
    seen = dot(after, flag((r0 == ej) | (r1c == ej)), 1, 0)
    arrived(ph.at[pl.ds(0, slots - 1)], pz_recv)
    table = jnp.concatenate([ph[i] for i in range(slots)], axis=0)
    for k in range(2):
        mine = (r0, r1c)[k] == ej
        rank = jnp.sum(jnp.where(mine, seen, 0.0), axis=1, keepdims=True)
        found = dot(jnp.where(mine, 1.0, 0.0), table, 1, 0, HIGH)
        lane = iota((n_tok, 128), 1).astype(F32)
        value = jnp.sum(jnp.where(lane == rank, found, 0.0), axis=1, keepdims=True)
        row = jnp.broadcast_to(value, (n_tok, n_tok)).T[0:1]
        wg_o[k : k + 1, :] = row / wt[k : k + 1, :]
    arrived(rh.at[:, pl.ds(0, (slots - 1) * pairs)], rz_recv)
    rhv = rh.reshape(2, rows, 128)
    for h in range(2):
        tg_o[:, h * 128 : (h + 1) * 128] = dot(cm[...], rhv[h], 1, 0).astype(BF)

    left(sb.at[:, pl.ds(0, (slots - 1) * pairs)], z_send)
    left(xa.at[:, pl.ds(0, n_tp - 1)], ag_send)
    left(r1, rs_send.at[0])
    left(r2, rs_send.at[1])
    left(rh.at[:, pl.ds(0, (slots - 1) * pairs)], rz_send)
    left(pb.at[pl.ds(0, n_tp - 1)], pb_send)
    left(ph.at[pl.ds(0, slots - 1)], pz_send)
    left(sc, sc_send)
    for way, hops in ((0, far), (1, far - 1)):
        for step in range(hops):
            left(shs.at[way, step], sh_send.at[way, step])


def settle(*refs):
    n = len(refs) // 3
    src, dst, held, sems = refs[:n], refs[n : 2 * n], refs[2 * n : 3 * n], refs[3 * n :]
    into = [pltpu.make_async_copy(src[i], held[i], sems[0].at[i]) for i in range(n)]
    out = [pltpu.make_async_copy(held[i], dst[i], sems[1].at[i]) for i in range(n)]
    for copy in into:
        copy.start()
    for i in range(n):
        into[i].wait()
        out[i].start()
    for copy in out:
        copy.wait()


def local(zs, tokens, out_grad, routes, route_weights, gate_proj, up_proj, down_proj, shared_hidden):
    n_tok, feat = tokens.shape
    _, fe, width = gate_proj.shape
    slots = 2 * zs
    cap = max(2, 5 * n_tok * routes.shape[1] // (4 * slots))
    rows = slots * cap
    nch = len(chunks_of(zs))
    half = rows // nch
    n_tp = SIDE * SIDE
    share = shared_hidden.shape[1] // slots
    far = zs // 2
    vmem = pl.BlockSpec(memory_space=pltpu.VMEM)
    hbm = pl.BlockSpec(memory_space=pltpu.HBM)
    dma = pltpu.SemaphoreType.DMA
    V = pltpu.VMEM
    out = pl.pallas_call(
        functools.partial(kernel, zs, cap),
        out_shape=(
            jax.ShapeDtypeStruct((n_tok, feat), BF),
            jax.ShapeDtypeStruct((2, n_tok), F32),
            jax.ShapeDtypeStruct((fe, width), BF),
            jax.ShapeDtypeStruct((fe, width), BF),
            jax.ShapeDtypeStruct((fe, width), BF),
            jax.ShapeDtypeStruct((share, feat), F32),
        ),
        in_specs=[hbm] * 8,
        out_specs=(vmem,) * 6,
        scratch_shapes=[
            V((n_tok, feat), BF),
            V((n_tok, feat), BF),
            V((2, n_tok), jnp.int32),
            V((2, n_tok), F32),
            V(shared_hidden.shape, BF),
            V((2 * fe, width), BF),
            V((fe, width), BF),
            V((4, rows // 2, 2, 128), BF),
            V((nch, n_tp, 4, half // 2, 2, 128), BF),
            V((rows, 2 * fe), BF),
            V((rows, fe), BF),
            V((nch, 2 * fe, half), BF),
            V((nch, fe, half), BF),
            V((nch, 2, SIDE, SIDE, half, 128), BF),
            V((nch, 2, 6, 2, half, 128), BF),
            V((nch, 2, 2, 2, half, 128), BF),
            V((nch, 2, half, 128), F32),
            V((nch, 2, 3, half, 128), BF),
            V((nch, 2, 3, half, 128), BF),
            V((nch, 2, half // 2, 2, 128), BF),
            V((2, rows // 2, 2, 128), BF),
            V((n_tp, nch, (half + 127) // 128 * 128), F32),
            V((slots, 1, 128), F32),
            V((slots, 1, 128), F32),
            V((n_tok, rows), BF),
            V((zs, 2, share, feat), F32),
            V((zs, share, feat), F32),
            V((2, far, share, feat), F32),
            V((2, far, share, feat), F32),
            V((half, 2 * fe), F32),
            V((half, fe), F32),
            dma((8,)),
            dma, dma((nch,)),
            dma, dma((nch, 2, 5, 4)),
            dma((2,)), dma((nch, 2, 9)),
            dma, dma,
            dma, dma,
            dma, dma,
            dma, dma,
            dma((2, far)), dma((2, far)),
        ],
        compiler_params=pltpu.CompilerParams(collective_id=0, has_side_effects=True, vmem_limit_bytes=60 * 1024 * 1024),
    )(
        tokens, out_grad, routes.T, route_weights.T,
        gate_proj[0], up_proj[0], down_proj[0], shared_hidden,
    )
    shapes = [jax.ShapeDtypeStruct(a.shape, a.dtype) for a in out]
    tg, wg, gg, ug, dg, sg = pl.pallas_call(
        settle,
        out_shape=shapes,
        in_specs=[hbm] * len(out),
        out_specs=[hbm] * len(out),
        scratch_shapes=[V(a.shape, a.dtype) for a in out] + [dma((len(out),)), dma((len(out),))],
    )(*out)
    return tg, wg.T, gg[None], ug[None], dg[None], sg


def solution(mesh):
    zs = mesh.shape["ep"] // 2
    features, whole, weights = P("ep", "tp"), P("ep", None), P("ep", "tp", None)
    return jax.shard_map(
        functools.partial(local, zs),
        mesh=mesh,
        in_specs=(features, features, whole, whole, weights, weights, weights, whole),
        out_specs=(features, whole, weights, weights, weights, features),
        check_vma=False,
    )
```

```python
import functools

import jax
import jax.numpy as jnp
from jax import lax
from jax.experimental import pallas as pl
from jax.experimental.pallas import tpu as pltpu
from jax.sharding import PartitionSpec as P

MESH = pl.DeviceIdType.MESH
BF = jnp.bfloat16
F32 = jnp.float32
SIDE = 4
ORDER = (0, 3, 2, 1)
HIGH = lax.Precision.HIGHEST


def chunks_of(zs):
    near = sorted(range(1 - zs // 2, zs // 2 + 1), key=lambda d: (abs(d), -d))
    size = zs // len(ORDER)
    parts = [near[k * size : (k + 1) * size] for k in range(len(ORDER))]
    return [parts[k] for k in ORDER]


def dot(a, b, da, db, precision=None):
    return lax.dot_general(
        a, b, (((da,), (db,)), ((), ())), preferred_element_type=F32, precision=precision
    )


def iota(shape, dim):
    return lax.broadcasted_iota(jnp.int32, shape, dim)


def kernel(
    zs, cap,
    tok_h, og_h, routes_h, rw_h, gate, up, down, sh_h,
    tg_o, wg_o, gg_h, ug_h, dg_h, sg_o,
    gg_o, ug_o, dg_o, g_sem, tok, og, routes_t, rw_t, sh, wgu, wdn, sb, xa, dl, hd, dlt, hdt, pr, r1, f1, s0, s1, r2, rt, rh, pb, pz, ph, cm,
    sp, sc, shb, shs, ea, eb,
    w_sem, z_send, z_recv, ag_send, ag_recv, rs_send, rs_recv, rz_send, rz_recv,
    pb_send, pb_recv, pz_send, pz_recv, sc_send, sc_recv, sh_send, sh_recv,
):
    ep, tp = lax.axis_index("ep"), lax.axis_index("tp")
    z, c = ep // 2, lax.rem(ep, 2)
    yx = (tp // SIDE, lax.rem(tp, SIDE))
    n_tp = SIDE * SIDE
    slots = 2 * zs
    rows = slots * cap
    groups = chunks_of(zs)
    nch = len(groups)
    ns = slots // nch
    half = rows // nch
    pairs = cap // 2
    fe = gate.shape[0]
    n_tok = tok.shape[0]

    def ring(d):
        return lax.rem(z + d + zs, zs)

    def ep_of(d, cd):
        return ring(d) * 2 + lax.rem(c + cd, 2)

    def tp_of(h, dp, ds):
        dy, dx = (ds, dp) if h == 0 else (dp, ds)
        return lax.rem(yx[0] + dy + SIDE, SIDE) * SIDE + lax.rem(yx[1] + dx + SIDE, SIDE)

    def remote(src, dst, ssem, rsem, dev):
        return pltpu.make_async_remote_copy(
            src_ref=src, dst_ref=dst, send_sem=ssem, recv_sem=rsem,
            device_id=dev, device_id_type=MESH,
        )

    def arrived(ref, sem):
        remote(ref, ref, sem, sem, (ep, tp)).wait_recv()

    def left(ref, sem):
        remote(ref, ref, sem, sem, (ep, tp)).wait_send()

    loads = [
        pltpu.make_async_copy(gate, wgu.at[pl.ds(0, fe)], w_sem.at[0]),
        pltpu.make_async_copy(up, wgu.at[pl.ds(fe, fe)], w_sem.at[1]),
        pltpu.make_async_copy(down, wdn, w_sem.at[2]),
    ]
    small = [
        pltpu.make_async_copy(src, dst, w_sem.at[3 + i])
        for i, (src, dst) in enumerate(
            ((routes_h, routes_t), (rw_h, rw_t), (tok_h, tok), (og_h, og), (sh_h, sh))
        )
    ]
    for load in small + loads:
        load.start()

    barrier = pltpu.get_barrier_semaphore()
    for d in range(zs):
        for cd in range(2):
            if d or cd:
                pl.semaphore_signal(barrier, inc=1, device_id=(ep_of(d, cd), tp), device_id_type=MESH)
    for dy in range(SIDE):
        for dx in range(SIDE):
            if dy or dx:
                pl.semaphore_signal(barrier, inc=1, device_id=(ep, tp_of(0, dx, dy)), device_id_type=MESH)

    for load in small:
        load.wait()

    def tables(shape, dim):
        r = iota(shape, dim)
        j = lax.shift_right_logical(r * (65536 // cap + 1), 16)
        e = lax.bitwise_and(z + lax.shift_right_logical(j, 1), zs - 1) * 2 + lax.bitwise_and(c + j, 1)
        return e, (r - cap * j).astype(F32)

    def flag(m):
        return jnp.where(m, 1.0, 0.0).astype(BF)

    def weight(x):
        return x.astype(BF).astype(F32)

    before = flag(iota((n_tok, n_tok), 0) < iota((n_tok, n_tok), 1))
    after = flag(iota((n_tok, n_tok), 0) > iota((n_tok, n_tok), 1))
    e, s = tables((rows, n_tok), 0)
    first = routes_t[0:1, :] == e
    hit = first | (routes_t[1:2, :] == e)
    chosen = hit & (dot(flag(hit), before, 1, 0) == s)
    wt = weight(rw_t[...])
    slot_w = jnp.sum(jnp.where(chosen, jnp.where(first, wt[0:1, :], wt[1:2, :]), 0.0), axis=1, keepdims=True)
    pick = flag(chosen)
    sbv = sb.reshape(4, rows, 128)
    for g in range(2):
        sbv[g] = dot(pick, tok[:, g * 128 : (g + 1) * 128], 1, 0).astype(BF)
        sbv[2 + g] = (slot_w * dot(pick, og[:, g * 128 : (g + 1) * 128], 1, 0)).astype(BF)

    share = sg_o.shape[0]
    for b in range(sp.shape[0]):
        for cc in range(2):
            lo = (b * 2 + cc) * share
            if lo % 128 == 0:
                wide = dot(sh[:, lo : lo + 128], og[...], 0, 0)
            sp[b, cc] = wide[lo % 128 : lo % 128 + share]

    pl.semaphore_wait(barrier, slots - 1 + n_tp - 1)

    def slot_in(d, cd):
        return [g.index(d) for g in groups if d in g][0] * 2 + cd

    def exchange(chunk):
        for d in groups[chunk]:
            for cd in (1, 0):
                if d or cd:
                    j = (d % zs) * 2 + cd
                    remote(
                        sb.at[:, pl.ds(j * pairs, pairs)],
                        xa.at[chunk, tp, :, pl.ds(slot_in(d, cd) * pairs, pairs)],
                        z_send, z_recv.at[chunk], (ep_of(d, cd), tp),
                    ).start()

    for ch in range(nch):
        exchange(ch)
    xa[0, tp, :, pl.ds(slot_in(0, 0) * pairs, pairs)] = sb[:, pl.ds(0, pairs)]

    remote(sp.at[:, 1 - c], sc, sc_send, sc_recv, (ep_of(0, 1), tp)).start()

    def term(d):
        zz = ring(d)
        return sp[zz, c] + sc[zz]

    far = zs // 2

    def shared(step):
        if step == 0:
            arrived(sc, sc_recv)
        for way, hops in ((0, far), (1, far - 1)):
            sign = 1 if way == 0 else -1
            if step > hops:
                continue
            total = term(sign * (hops - step))
            if step:
                arrived(shb.at[way, step - 1], sh_recv.at[way, step - 1])
                total = total + shb[way, step - 1]
            if step < hops:
                shs[way, step] = total
                remote(
                    shs.at[way, step], shb.at[way, step], sh_send.at[way, step], sh_recv.at[way, step],
                    (ep_of(sign, 0), tp),
                ).start()
            elif way == 1:
                sg_o[...] = total
            else:
                sg_o[...] = sg_o[...] + total - term(0)

    back = (0, -1, 1, 2)

    def gather_send(ch, h, k, kind, t, g0, gn, dev_t):
        ref = xa.at[ch, t, pl.ds(2 * h + g0, gn)]
        remote(ref, ref, ag_send, ag_recv.at[ch, h, k, kind], (ep, dev_t)).start()

    def gather_wait(ch, h, k, kind, g0, gn):
        arrived(xa.at[ch, 0, pl.ds(2 * h + g0, gn)], ag_recv.at[ch, h, k, kind])

    def spread(ch, h, k):
        t = tp_of(h, back[k], 0)
        gather_send(ch, h, k, 0, t, 0, 2, tp_of(h, 0, 1))
        gather_send(ch, h, k, 1, t, 0, 2, tp_of(h, 0, -1))

    def relay(ch, h, k):
        gather_wait(ch, h, k, 0, 0, 2)
        gather_send(ch, h, k, 2, tp_of(h, back[k], -1), 0, 1, tp_of(h, 0, 1))
        gather_wait(ch, h, k, 1, 0, 2)
        gather_send(ch, h, k, 3, tp_of(h, back[k], 1), 1, 1, tp_of(h, 0, -1))

    def g_0(ch):
        arrived(xa.at[ch, 0, :, pl.ds(0, (ns - (1 if ch == 0 else 0)) * pairs)], z_recv.at[ch])
        for h in range(2):
            gather_send(ch, h, 4, 0, tp, 0, 2, tp_of(h, 1, 0))
            gather_send(ch, h, 4, 1, tp, 0, 2, tp_of(h, -1, 0))
        for h in range(2):
            spread(ch, h, 0)

    def g_1(ch):
        for h in range(2):
            gather_wait(ch, h, 4, 0, 0, 2)
            gather_send(ch, h, 4, 2, tp_of(h, -1, 0), 0, 1, tp_of(h, 1, 0))
            gather_wait(ch, h, 4, 1, 0, 2)
            gather_send(ch, h, 4, 3, tp_of(h, 1, 0), 1, 1, tp_of(h, -1, 0))
        for h in range(2):
            spread(ch, h, 1)
            spread(ch, h, 2)

    def g_2(ch):
        for h in range(2):
            relay(ch, h, 0)
        for h in range(2):
            gather_wait(ch, h, 4, 2, 0, 1)
            gather_wait(ch, h, 4, 3, 1, 1)
            spread(ch, h, 3)

    def g_3(ch):
        for h in range(2):
            relay(ch, h, 1)
            relay(ch, h, 2)

    def g_4(ch):
        for h in range(2):
            relay(ch, h, 3)

    def g_5(ch, ks=range(4)):
        for h in range(2):
            for k in ks:
                gather_wait(ch, h, k, 2, 0, 1)
                gather_wait(ch, h, k, 3, 1, 1)

    xav = xa.reshape(nch, n_tp, 4, half, 128)
    width = 256

    def early(ch, dps, start):
        a, b = start
        for dp in dps:
            for ds in range(SIDE):
                t, u = tp_of(0, dp, ds), tp_of(1, dp, ds)
                x = jnp.concatenate([xav[ch, t, 0], xav[ch, t, 1]], axis=1)
                y = jnp.concatenate([xav[ch, u, 2], xav[ch, u, 3]], axis=1)
                a = a + dot(x, wgu[:, pl.ds(pl.multiple_of(t * width, width), width)], 1, 1)
                b = b + dot(y, wdn[:, pl.ds(pl.multiple_of(u * width, width), width)], 1, 1)
        return a, b

    def expert_early(ch):
        start = (jnp.zeros((half, 2 * fe), F32), jnp.zeros((half, fe), F32))
        ea[...], eb[...] = early(ch, (0, -1, 1), start)

    def expert(ch, late=False):
        def sums(i, total):
            a, b = total
            for u in range(4):
                t = i * 4 + u
                cols = pl.ds(pl.multiple_of(t * width, width), width)
                x = jnp.concatenate([xav[ch, t, 0], xav[ch, t, 1]], axis=1)
                y = jnp.concatenate([xav[ch, t, 2], xav[ch, t, 3]], axis=1)
                a = a + dot(x, wgu[:, cols], 1, 1)
                b = b + dot(y, wdn[:, cols], 1, 1)
            return a, b

        start = (jnp.zeros((half, 2 * fe), F32), jnp.zeros((half, fe), F32))
        if late:
            gu, back_grad = early(ch, (2,), (ea[...], eb[...]))
        else:
            gu, back_grad = lax.fori_loop(0, n_tp // 4, sums, start)
        pre_gate, pre_up = gu[:, :fe], gu[:, fe:]
        squash = 1.0 / (1.0 + jnp.exp(-pre_gate))
        activated = pre_gate * squash
        hidden = (activated * pre_up).astype(BF)
        gate_delta = back_grad * pre_up * squash * (1.0 + pre_gate * (1.0 - squash))
        at = pl.ds(ch * half, half)
        deltas = jnp.concatenate([gate_delta, back_grad * activated], axis=1)
        dl[at, :] = deltas.astype(BF)
        hd[at, :] = hidden
        product = hidden.astype(F32) * back_grad
        line = dot(jnp.ones((8, fe), F32), product, 1, 1, HIGH)
        pb[tp, pl.ds(ch, 1), pl.ds(0, half)] = line[0:1]

    def parts(ch, which=(True, False)):
        at = pl.ds(ch * half, half)
        for dy in range(SIDE):
            for dx in range(SIDE):
                if (2 in (dx, dy)) not in which:
                    continue
                t = tp_of(0, dx, dy)
                cols = pl.ds(pl.multiple_of(t * width, width), width)
                out = dot(dl[at, :], wgu[:, cols], 1, 0).astype(BF)
                pr[ch, 0, dx, dy] = out[:, :128]
                pr[ch, 1, dy, dx] = out[:, 128:]

    def add(*xs):
        total = xs[0].astype(F32)
        for x in xs[1:]:
            total = total + x.astype(F32)
        return total

    def landing(ch, h, i, base):
        return (r1 if base == 0 else r2).at[ch, h, i]

    def sum_send(ch, h, src, i, base, dev_t):
        remote(src, landing(ch, h, i, base), rs_send.at[base // 6], rs_recv.at[ch, h, base + i], (ep, dev_t)).start()

    def sum_wait(ch, h, i, base):
        arrived(landing(ch, h, i, base), rs_recv.at[ch, h, base + i])

    lo, hi = pl.ds(0, 2), pl.ds(2, 2)

    def q_0(ch):
        q_0a(ch)
        q_0b(ch)

    def q_0a(ch):
        for h in range(2):
            sum_send(ch, h, pr.at[ch, h, 2, lo], 0, 0, tp_of(h, 1, 0))
            sum_send(ch, h, pr.at[ch, h, 2, hi], 1, 0, tp_of(h, -1, 0))

    def q_0b(ch):
        for h in range(2):
            sum_send(ch, h, pr.at[ch, h, 1, hi], 2, 0, tp_of(h, 1, 0))
            sum_send(ch, h, pr.at[ch, h, 3, lo], 3, 0, tp_of(h, -1, 0))

    def q_1(ch):
        for h in range(2):
            sum_wait(ch, h, 0, 0)
            f1[ch, h, 0] = add(pr[ch, h, 1, lo], r1[ch, h, 0]).astype(BF)
            sum_send(ch, h, f1.at[ch, h, 0], 4, 0, tp_of(h, 1, 0))
            sum_wait(ch, h, 1, 0)
            f1[ch, h, 1] = add(pr[ch, h, 3, hi], r1[ch, h, 1]).astype(BF)
            sum_send(ch, h, f1.at[ch, h, 1], 5, 0, tp_of(h, -1, 0))

    def q_2(ch):
        for h in range(2):
            for i in (3, 2, 4, 5):
                sum_wait(ch, h, i, 0)
            for ds in (2, 1, 3, 0):
                pair = (4, 3) if ds < 2 else (2, 5)
                total = add(pr[ch, h, 0, ds], r1[ch, h, pair[0], ds % 2], r1[ch, h, pair[1], ds % 2])
                if ds:
                    s1[ch, h, ds - 1] = total.astype(BF)
                else:
                    s0[ch, h] = total
            for i, ds in ((1, 2), (0, 1), (2, -1)):
                sum_send(ch, h, s1.at[ch, h, i], i, 6, tp_of(h, 0, ds))

    rtv = rt.reshape(nch, 2, half, 128)

    def q_4(ch):
        for h in range(2):
            for i in (0, 2, 1):
                sum_wait(ch, h, i, 6)
            rtv[ch, h] = add(s0[ch, h], r2[ch, h, 0], r2[ch, h, 2], r2[ch, h, 1]).astype(BF)
        for d in groups[ch][::-1]:
            for cd in (1, 0):
                here = pl.ds(slot_in(d, cd) * pairs, pairs)
                there = pl.ds(((d % zs) * 2 + cd) * pairs, pairs)
                if d or cd:
                    remote(
                        rt.at[ch, :, here], rh.at[:, there], rz_send, rz_recv, (ep_of(-d, cd), tp)
                    ).start()
                else:
                    rh[:, there] = rt[ch, :, here]

    def product_send():
        for dy in range(SIDE):
            for dx in range(SIDE):
                if dy or dx:
                    remote(pb.at[tp], pb.at[tp], pb_send, pb_recv, (ep, tp_of(0, dx, dy))).start()

    def product_return():
        arrived(pb.at[pl.ds(0, n_tp - 1)], pb_recv)
        for ch in range(nch):
            total = pb[0, pl.ds(ch, 1), pl.ds(0, half)]
            for t in range(1, n_tp):
                total = total + pb[t, pl.ds(ch, 1), pl.ds(0, half)]
            r = iota((ns, half), 1)
            j = lax.shift_right_logical(r * (65536 // cap + 1), 16)
            own = jnp.where(j == iota((ns, half), 0), total, 0.0)
            r = iota((half, 128), 0)
            j = lax.shift_right_logical(r * (65536 // cap + 1), 16)
            lane = jnp.where(r - cap * j == iota((half, 128), 1), 1.0, 0.0)
            table = dot(own, lane, 1, 0, HIGH)
            for i in range(ns):
                pz[ch * ns + i] = table[i : i + 1]
        for ch in range(nch):
            for d in groups[ch][::-1]:
                for cd in (1, 0):
                    i, j = ch * ns + slot_in(d, cd), (d % zs) * 2 + cd
                    if d or cd:
                        remote(pz.at[i], ph.at[j], pz_send, pz_recv, (ep_of(-d, cd), tp)).start()
                    else:
                        ph[j] = pz[i]

    def weight_grads(t0, t1):
        def one(t, carry):
            cols = pl.ds(pl.multiple_of(t * width, width), width)
            both = jnp.zeros((2 * fe, width), F32)
            last = jnp.zeros((fe, width), F32)
            for ch in range(nch):
                x = jnp.concatenate([xav[ch, t, 0], xav[ch, t, 1]], axis=1)
                y = jnp.concatenate([xav[ch, t, 2], xav[ch, t, 3]], axis=1)
                both = both + dot(dlt[ch], x, 1, 0)
                last = last + dot(hdt[ch], y, 1, 0)
            gg_o[:, cols] = both[:fe].astype(BF)
            ug_o[:, cols] = both[fe:].astype(BF)
            dg_o[:, cols] = last.astype(BF)
            return carry

        lax.fori_loop(t0, t1, one, 0)

    def turned(ch):
        at = pl.ds(ch * half, half)
        dlt[ch] = dl[at, :].astype(F32).T.astype(BF)
        hdt[ch] = hd[at, :].astype(F32).T.astype(BF)

    shared(0)
    g_0(0)
    g_1(0)
    g_2(0)
    g_0(1)
    g_3(0)
    g_1(1)
    g_0(2)
    g_4(0)
    g_0(3)
    shared(1)
    g_2(1)
    g_1(2)
    g_5(0)
    for load in loads:
        load.wait()
    expert(0)
    shared(2)
    g_1(3)
    g_3(1)
    g_2(2)
    shared(3)
    parts(0)
    g_4(1)
    g_2(3)
    g_3(2)
    shared(4)
    g_5(1)
    g_3(3)
    g_4(2)
    expert(1)
    shared(5)
    g_4(3)
    q_0(0)
    parts(1)
    q_0(1)
    g_5(2)
    shared(6)
    expert(2)
    q_1(0)
    parts(2)
    q_0(2)
    q_1(1)
    g_5(3, (0, 1, 2))
    shared(7)
    expert_early(3)
    g_5(3, (3,))
    expert(3, True)
    parts(3, (True,))
    q_0a(3)
    parts(3, (False,))
    q_0b(3)
    product_send()
    q_2(0)
    q_1(2)
    q_2(1)
    q_1(3)
    shared(8)
    q_4(0)
    turned(0)
    turned(1)
    q_2(2)
    q_4(1)
    q_2(3)
    turned(2)
    turned(3)
    weight_grads(0, 1)
    product_return()
    q_4(2)
    weight_grads(1, 2)
    q_4(3)
    weight_grads(2, 16)

    e, s = tables((n_tok, rows), 1)
    def turn(row):
        return jnp.broadcast_to(row, (n_tok, n_tok)).T

    r0, r1c = (turn(routes_t[k : k + 1, :].astype(F32))[:, 0:1].astype(jnp.int32) for k in range(2))
    hit = (r0 == e) | (r1c == e)
    cm[...] = flag(hit & (dot(after, flag(hit), 1, 0) == s))
    j = iota((n_tok, slots), 1)
    ej = lax.bitwise_and(z + lax.shift_right_logical(j, 1), zs - 1) * 2 + lax.bitwise_and(c + j, 1)
    seen = dot(after, flag((r0 == ej) | (r1c == ej)), 1, 0)
    stores = [
        pltpu.make_async_copy(src, dst, g_sem.at[i])
        for i, (src, dst) in enumerate(((gg_o, gg_h), (ug_o, ug_h), (dg_o, dg_h)))
    ]
    for store in stores:
        store.start()
    arrived(ph.at[pl.ds(0, slots - 1)], pz_recv)
    table = jnp.concatenate([ph[i] for i in range(slots)], axis=0)
    for k in range(2):
        mine = (r0, r1c)[k] == ej
        rank = jnp.sum(jnp.where(mine, seen, 0.0), axis=1, keepdims=True)
        found = dot(jnp.where(mine, 1.0, 0.0), table, 1, 0, HIGH)
        lane = iota((n_tok, 128), 1).astype(F32)
        value = jnp.sum(jnp.where(lane == rank, found, 0.0), axis=1, keepdims=True)
        row = jnp.broadcast_to(value, (n_tok, n_tok)).T[0:1]
        wg_o[k : k + 1, :] = row / wt[k : k + 1, :]
    arrived(rh.at[:, pl.ds(0, (slots - 1) * pairs)], rz_recv)
    rhv = rh.reshape(2, rows, 128)
    for h in range(2):
        tg_o[:, h * 128 : (h + 1) * 128] = dot(cm[...], rhv[h], 1, 0).astype(BF)

    for store in stores:
        store.wait()
    left(sb.at[:, pl.ds(0, (slots - 1) * pairs)], z_send)
    left(xa.at[:, pl.ds(0, n_tp - 1)], ag_send)
    left(r1, rs_send.at[0])
    left(r2, rs_send.at[1])
    left(rh.at[:, pl.ds(0, (slots - 1) * pairs)], rz_send)
    left(pb.at[pl.ds(0, n_tp - 1)], pb_send)
    left(ph.at[pl.ds(0, slots - 1)], pz_send)
    left(sc, sc_send)
    for way, hops in ((0, far), (1, far - 1)):
        for step in range(hops):
            left(shs.at[way, step], sh_send.at[way, step])


def settle(*refs):
    n = len(refs) // 3
    src, dst, held, sems = refs[:n], refs[n : 2 * n], refs[2 * n : 3 * n], refs[3 * n :]
    into = [pltpu.make_async_copy(src[i], held[i], sems[0].at[i]) for i in range(n)]
    out = [pltpu.make_async_copy(held[i], dst[i], sems[1].at[i]) for i in range(n)]
    for copy in into:
        copy.start()
    for i in range(n):
        into[i].wait()
        out[i].start()
    for copy in out:
        copy.wait()


def local(zs, tokens, out_grad, routes, route_weights, gate_proj, up_proj, down_proj, shared_hidden):
    n_tok, feat = tokens.shape
    _, fe, width = gate_proj.shape
    slots = 2 * zs
    cap = max(2, 5 * n_tok * routes.shape[1] // (4 * slots))
    rows = slots * cap
    nch = len(chunks_of(zs))
    half = rows // nch
    n_tp = SIDE * SIDE
    share = shared_hidden.shape[1] // slots
    far = zs // 2
    vmem = pl.BlockSpec(memory_space=pltpu.VMEM)
    hbm = pl.BlockSpec(memory_space=pltpu.HBM)
    dma = pltpu.SemaphoreType.DMA
    V = pltpu.VMEM
    out = pl.pallas_call(
        functools.partial(kernel, zs, cap),
        out_shape=(
            jax.ShapeDtypeStruct((n_tok, feat), BF),
            jax.ShapeDtypeStruct((2, n_tok), F32),
            jax.ShapeDtypeStruct((fe, width), BF),
            jax.ShapeDtypeStruct((fe, width), BF),
            jax.ShapeDtypeStruct((fe, width), BF),
            jax.ShapeDtypeStruct((share, feat), F32),
        ),
        in_specs=[hbm] * 8,
        out_specs=(vmem, vmem, hbm, hbm, hbm, vmem),
        scratch_shapes=[
            V((fe, width), BF),
            V((fe, width), BF),
            V((fe, width), BF),
            dma((3,)),
            V((n_tok, feat), BF),
            V((n_tok, feat), BF),
            V((2, n_tok), jnp.int32),
            V((2, n_tok), F32),
            V(shared_hidden.shape, BF),
            V((2 * fe, width), BF),
            V((fe, width), BF),
            V((4, rows // 2, 2, 128), BF),
            V((nch, n_tp, 4, half // 2, 2, 128), BF),
            V((rows, 2 * fe), BF),
            V((rows, fe), BF),
            V((nch, 2 * fe, half), BF),
            V((nch, fe, half), BF),
            V((nch, 2, SIDE, SIDE, half, 128), BF),
            V((nch, 2, 6, 2, half, 128), BF),
            V((nch, 2, 2, 2, half, 128), BF),
            V((nch, 2, half, 128), F32),
            V((nch, 2, 3, half, 128), BF),
            V((nch, 2, 3, half, 128), BF),
            V((nch, 2, half // 2, 2, 128), BF),
            V((2, rows // 2, 2, 128), BF),
            V((n_tp, nch, (half + 127) // 128 * 128), F32),
            V((slots, 1, 128), F32),
            V((slots, 1, 128), F32),
            V((n_tok, rows), BF),
            V((zs, 2, share, feat), F32),
            V((zs, share, feat), F32),
            V((2, far, share, feat), F32),
            V((2, far, share, feat), F32),
            V((half, 2 * fe), F32),
            V((half, fe), F32),
            dma((8,)),
            dma, dma((nch,)),
            dma, dma((nch, 2, 5, 4)),
            dma((2,)), dma((nch, 2, 9)),
            dma, dma,
            dma, dma,
            dma, dma,
            dma, dma,
            dma((2, far)), dma((2, far)),
        ],
        compiler_params=pltpu.CompilerParams(collective_id=0, has_side_effects=True, vmem_limit_bytes=60 * 1024 * 1024),
    )(
        tokens, out_grad, routes.T, route_weights.T,
        gate_proj[0], up_proj[0], down_proj[0], shared_hidden,
    )
    shapes = [jax.ShapeDtypeStruct(a.shape, a.dtype) for a in out]
    tg, wg, gg, ug, dg, sg = pl.pallas_call(
        settle,
        out_shape=shapes,
        in_specs=[hbm] * len(out),
        out_specs=[hbm] * len(out),
        scratch_shapes=[V(a.shape, a.dtype) for a in out] + [dma((len(out),)), dma((len(out),))],
    )(*out)
    return tg, wg.T, gg[None], ug[None], dg[None], sg


def solution(mesh):
    zs = mesh.shape["ep"] // 2
    features, whole, weights = P("ep", "tp"), P("ep", None), P("ep", "tp", None)
    return jax.shard_map(
        functools.partial(local, zs),
        mesh=mesh,
        in_specs=(features, features, whole, whole, weights, weights, weights, whole),
        out_specs=(features, whole, weights, weights, weights, features),
        check_vma=False,
    )
```
